32 devices in a mesh: sp: 16 (over z, y, x), tp: 2 (over core).
Axes of the slice: x: 2, y: 2, z: 4, core: 2. Of those that a mesh axis runs over, the one named last changes fastest.
Arguments:
- queries: bfloat16 [4096, 2048], P('sp', 'tp'), may hold values from -6 to 6
- keys: bfloat16 [4096, 2048], P('sp', 'tp'), may hold values from -6 to 6
- hidden: bfloat16 [4096, 2048], P('sp'), may hold values from -6 to 6
- value_weight: bfloat16 [2048, 2048], P(None, 'tp'), may hold values from -0.125 to 0.125
- beta_pre: float32 [4096, 16], P('sp', 'tp'), may hold values from -9 to 3
- decay_pre: float32 [4096, 16], P('sp', 'tp'), may hold values from -5 to 4
- decay_rate: float32 [16], P('tp'), may hold values from 0 to 0.06
- out_grad: bfloat16 [4096, 2048], P('sp', 'tp'), may hold values from -6 to 6
Outputs:
- d_queries: bfloat16 [4096, 2048], P('sp', 'tp')
- d_keys: bfloat16 [4096, 2048], P('sp', 'tp')
- d_beta: float32 [4096, 16], P('sp', 'tp')
- d_decay: float32 [4096, 16], P('sp', 'tp')
- d_hidden: bfloat16 [4096, 2048], P(('sp', 'tp'))
- d_weight: float32 [2048, 2048], P('sp', 'tp')
The draws below stay inside these ranges and needn't reach their ends.
All inputs are finite; a program needn't handle non-finite values.
Results may differ from the reference program's by a relative error of at most 0.022.
Values may be sent and summed in bfloat16 or wider, within the bound.
No kernel may reach another device: no remote copies, remote signals or barrier semaphores. Data moves between devices by JAX's collectives and lax.ppermute only.
A program may use at most 256 MiB of HBM per device.

```python
import jax
import jax.numpy as jnp
from jax import lax

D = 2048
HEADS = 16
DK = 128
DV = 128
BLOCK = 64
TOK_DEV = 256
TOKENS = 4096
HEADS_DEV = 8


def slow_heads(key):
    order = jax.random.permutation(jax.random.fold_in(key, 11), HEADS)
    return order < HEADS // 2


def noise_field(key, shape):
    return jnp.clip(jax.random.normal(key, shape, jnp.float32), -3.0, 3.0)


def draw_decay_rate(key, part):
    slow = slow_heads(key)
    pick = jax.random.uniform(jax.random.fold_in(key, 12), (HEADS,), jnp.float32)
    return jnp.where(slow, (0.3 + 1.2 * pick) / TOKENS, 0.02 + 0.04 * pick)


def draw_beta_pre(key, part):
    slow = slow_heads(key)
    noise = noise_field(jax.random.fold_in(key, 13), (TOKENS, HEADS))
    return noise + jnp.where(slow, -5.5, 0.0)[None, :]


def draw_decay_pre(key, part):
    offset = jax.random.uniform(jax.random.fold_in(key, 21), (TOKENS // TOK_DEV, HEADS), jnp.float32, -2.0, 1.0)
    noise = noise_field(jax.random.fold_in(key, 22), (TOKENS, HEADS))
    return noise + jnp.repeat(offset, TOK_DEV, axis=0)


def shard_levels(key, dims, cuts, least, high):
    loudness = 1.0
    for dim, blocks in cuts:
        steps = jax.random.uniform(jax.random.fold_in(jax.random.fold_in(key, 6), dim), (blocks,), jnp.float32, least / len(cuts), high / len(cuts))
        loudness = loudness * jnp.repeat(jnp.exp(steps), dims[dim] // blocks).reshape((-1,) + (1,) * (len(dims) - 1 - dim))
    return loudness


def normal_values(stream_key, extent, scale, reach, cuts=(), kind=jnp.bfloat16):
    factor_of = shard_levels(stream_key, extent, cuts, -0.22, 0.18) if cuts else 1.0
    array = jax.random.normal(stream_key, extent, jnp.float32) * scale * factor_of
    return jnp.minimum(jnp.maximum(array, -reach), reach).astype(kind)


def setup_inputs(seed: int = 0) -> dict:
    arg_keys = jax.random.split(jax.random.key(seed), 9)
    return {
        "queries": normal_values(arg_keys[0], (TOKENS, HEADS * DK), 1.0, 6.0, ((0, 16), (1, 2))),
        "keys": normal_values(arg_keys[1], (TOKENS, HEADS * DK), 1.0, 6.0, ((0, 16), (1, 2))),
        "hidden": normal_values(arg_keys[2], (TOKENS, D), 1.0, 6.0, ((0, 16),)),
        "value_weight": normal_values(arg_keys[3], (D, HEADS * DV), D ** -0.5, 0.125, ((1, 2),)),
        "beta_pre": draw_beta_pre(jax.random.fold_in(arg_keys[8], 71), 0),
        "decay_pre": draw_decay_pre(jax.random.fold_in(arg_keys[8], 71), 0),
        "decay_rate": draw_decay_rate(jax.random.fold_in(arg_keys[8], 71), 0),
        "out_grad": normal_values(arg_keys[7], (TOKENS, HEADS * DV), 1.0, 6.0, ((0, 16), (1, 2))),
    }


highest = lax.Precision.HIGHEST
norm_floor = 16.0

def to_blocks(tensor, blocks):
    shaped = tensor.reshape((blocks, BLOCK) + tensor.shape[1:])
    return jnp.moveaxis(shaped, 1, 2)

def block_setup(key_raw, beta_pre, decay_pre, rate):
    blocks = key_raw.shape[0] // BLOCK
    key_unit = key_raw * lax.rsqrt(lax.optimization_barrier(jnp.sum(key_raw * key_raw, axis=-1, keepdims=True)) + norm_floor)
    write_rate = jax.nn.sigmoid(beta_pre)
    log_decay = -rate[None, :] * jax.nn.softplus(decay_pre)
    key_blocks = to_blocks(key_unit, blocks)
    rate_blocks = to_blocks(write_rate, blocks)
    log_sums = jnp.cumsum(to_blocks(log_decay, blocks), axis=-1)
    position = jnp.arange(BLOCK)
    inclusive = position[:, None] >= position[None, :]
    strict = position[:, None] > position[None, :]
    spread = log_sums[..., :, None] - log_sums[..., None, :]
    decay_mask = jnp.where(inclusive, jnp.exp(jnp.where(inclusive, spread, 0.0)), 0.0)
    key_gram = jnp.einsum('nhid,nhjd->nhij', key_blocks, key_blocks, precision=highest)
    lower_part = jnp.where(strict, rate_blocks[..., :, None] * key_gram * decay_mask, 0.0)
    system = jnp.eye(BLOCK, dtype=jnp.float32) + lower_part
    return (key_blocks, rate_blocks, log_sums, decay_mask, system)

def span_pieces(query_raw, key_raw, values, beta_pre, decay_pre, rate):
    key_blocks, rate_blocks, log_sums, decay_mask, system = block_setup(key_raw, beta_pre, decay_pre, rate)
    blocks = key_blocks.shape[0]
    query_unit = query_raw * lax.rsqrt(lax.optimization_barrier(jnp.sum(query_raw * query_raw, axis=-1, keepdims=True)) + norm_floor)
    query_unit = query_unit * query_raw.shape[-1] ** (-0.5)
    query_blocks = to_blocks(query_unit, blocks)
    value_blocks = to_blocks(values, blocks)
    block_gain = jnp.exp(log_sums)
    right_side = jnp.concatenate([rate_blocks[..., None] * value_blocks, (rate_blocks * block_gain)[..., None] * key_blocks], axis=-1)
    solved = jax.scipy.linalg.solve_triangular(system, right_side, lower=True, unit_diagonal=True)
    value_size = values.shape[-1]
    query_key = jnp.einsum('nhid,nhjd->nhij', query_blocks, key_blocks, precision=highest) * decay_mask
    query_decayed = query_blocks * block_gain[..., None]
    key_decayed = key_blocks * jnp.exp(log_sums[..., -1:] - log_sums)[..., None]
    return (solved[..., :value_size], solved[..., value_size:], query_key, query_decayed, key_decayed, block_gain[..., -1])

def span_run(query_raw, key_raw, values, beta_pre, decay_pre, rate, carry_state):
    pieces = span_pieces(query_raw, key_raw, values, beta_pre, decay_pre, rate)

    def advance(current, inputs):
        new_values, key_sweep, query_key, query_decayed, key_decayed, end_gain = inputs
        written = new_values - jnp.einsum('hcd,hde->hce', key_sweep, current, precision=highest)
        output = jnp.einsum('hcd,hde->hce', query_decayed, current, precision=highest)
        output = output + jnp.einsum('hij,hje->hie', query_key, written, precision=highest)
        current = end_gain[:, None, None] * current + jnp.einsum('hcd,hce->hde', key_decayed, written, precision=highest)
        return (current, output)
    final, outputs = lax.scan(advance, carry_state, pieces)
    outputs = jnp.moveaxis(outputs, 2, 1)
    return (outputs.reshape(query_raw.shape[0], outputs.shape[2], outputs.shape[3]), final)

def reference(queries, keys, hidden, value_weight, beta_pre, decay_pre, decay_rate, out_grad):
    values = jnp.dot(hidden.astype(jnp.float32), value_weight.astype(jnp.float32), preferred_element_type=jnp.float32).astype(jnp.bfloat16)
    spans = TOKENS // TOK_DEV

    def by_span(tensor, width):
        return tensor.astype(jnp.float32).reshape(spans, TOK_DEV, HEADS, width)
    query_spans = by_span(queries, DK)
    key_spans = by_span(keys, DK)
    value_spans = by_span(values, DV)
    grad_spans = by_span(out_grad, DV)
    beta_spans = beta_pre.reshape(spans, TOK_DEV, HEADS)
    decay_spans = decay_pre.reshape(spans, TOK_DEV, HEADS)
    zero_state = jnp.zeros((HEADS, DK, DV), jnp.float32)

    def local_run(query_raw, key_raw, span_values, span_beta, span_decay, start_state):
        return span_run(query_raw, key_raw, span_values, span_beta, span_decay, decay_rate, start_state)

    def forward(current, inputs):
        outputs, final = local_run(*inputs, current)
        return (final, current)
    _, starts = lax.scan(forward, zero_state, (query_spans, key_spans, value_spans, beta_spans, decay_spans))

    def backward(state_grad, inputs):
        query_raw, key_raw, span_values, span_beta, span_decay, span_grad, start_state = inputs
        primal = (query_raw, key_raw, span_values, span_beta, span_decay)
        _, pullback = jax.vjp(local_run, *primal, start_state)
        grad_query, grad_key, grad_value, grad_beta, grad_decay, grad_state = pullback((span_grad, state_grad))
        _, pull_zero = jax.vjp(local_run, *primal, zero_state)
        own_value = pull_zero((span_grad, jnp.zeros_like(zero_state)))[2]
        return (grad_state, (grad_query, grad_key, grad_value, grad_beta, grad_decay, own_value))
    _, grads = lax.scan(backward, zero_state, (query_spans, key_spans, value_spans, beta_spans, decay_spans, grad_spans, starts), reverse=True)
    grad_query, grad_key, value_total, grad_beta, grad_decay, value_local = grads
    d_queries = grad_query.reshape(TOKENS, HEADS * DK).astype(jnp.bfloat16)
    d_keys = grad_key.reshape(TOKENS, HEADS * DK).astype(jnp.bfloat16)
    d_beta = grad_beta.reshape(TOKENS, HEADS)
    d_decay = grad_decay.reshape(TOKENS, HEADS)
    value_carried = value_total - value_local
    local_grad = value_local.reshape(TOKENS, HEADS * DV).astype(jnp.bfloat16)
    carried_grad = value_carried.reshape(TOKENS, HEADS * DV).astype(jnp.bfloat16)
    d_weight = jnp.dot(hidden.T.astype(jnp.float32), local_grad.astype(jnp.float32), preferred_element_type=jnp.float32)
    d_weight = d_weight + jnp.dot(hidden.T.astype(jnp.float32), carried_grad.astype(jnp.float32), preferred_element_type=jnp.float32)
    group_width = HEADS_DEV * DV
    total = jnp.zeros((TOKENS, D), jnp.float32)
    for group in range(HEADS // HEADS_DEV):
        columns = slice(group * group_width, (group + 1) * group_width)
        weight_part = value_weight[:, columns].T
        partial_sum = jnp.dot(local_grad[:, columns].astype(jnp.float32), weight_part.astype(jnp.float32), preferred_element_type=jnp.float32)
        partial_sum = partial_sum + jnp.dot(carried_grad[:, columns].astype(jnp.float32), weight_part.astype(jnp.float32), preferred_element_type=jnp.float32)
        rounded = lax.optimization_barrier(partial_sum.astype(jnp.bfloat16))
        total = total + rounded.astype(jnp.float32)
    d_hidden = total.astype(jnp.bfloat16)
    return (d_queries, d_keys, d_beta, d_decay, d_hidden, d_weight)
```

```python
import functools

import jax
import jax.numpy as jnp
from jax import lax
from jax.experimental import pallas as pl
from jax.experimental.pallas import tpu as pltpu
from jax.sharding import PartitionSpec as P

NORM_FLOOR = 16.0
F32 = jnp.float32
BF16 = jnp.bfloat16
HIGHEST = lax.Precision.HIGHEST
VMEM_LIMIT = 56 * 1024 * 1024


def dot(a, b, ca=1, cb=0, precision=None):
    return lax.dot_general(
        a, b, (((ca,), (cb,)), ((), ())), precision=precision, preferred_element_type=F32
    )


def low(x):
    return x.astype(BF16)


def iotas(n):
    rows = lax.broadcasted_iota(jnp.int32, (n, n), 0)
    cols = lax.broadcasted_iota(jnp.int32, (n, n), 1)
    return rows, cols


def head_columns(beta_pre, decay_pre, rate, g_ref, b_ref, gt_ref):
    n, heads = beta_pre.shape
    rows, cols = iotas(n)
    log_decay = -rate * (jnp.maximum(decay_pre, 0.0) + jnp.log1p(jnp.exp(-jnp.abs(decay_pre))))
    sums = dot((rows >= cols).astype(F32), log_decay, precision=HIGHEST)
    g_ref[...] = jnp.zeros_like(g_ref)
    b_ref[...] = jnp.zeros_like(b_ref)
    g_ref[:, 0:heads] = sums
    b_ref[:, 0:heads] = 1.0 / (1.0 + jnp.exp(-beta_pre))
    gt_ref[...] = jnp.transpose(g_ref[...])


def lane_column(ref, head):
    full = ref[...]
    width = full.shape[1]
    rolled = pltpu.roll(full, lax.rem(width - head, width), 1)
    return jnp.broadcast_to(rolled[:, 0:1], full.shape)


def head_common(q16, k16, head, g_ref, b_ref, gt_ref):
    n, size = k16.shape
    k32, q32 = k16.astype(F32), q16.astype(F32)
    g = lane_column(g_ref, head)
    beta = lane_column(b_ref, head)
    rk = jnp.broadcast_to(
        lax.rsqrt(jnp.sum(k32 * k32, axis=1, keepdims=True) + NORM_FLOOR), (n, size)
    )
    rq = jnp.broadcast_to(
        lax.rsqrt(jnp.sum(q32 * q32, axis=1, keepdims=True) + NORM_FLOOR), (n, size)
    )
    g_row = gt_ref[pl.ds(head, 1), :]
    rk_row = jnp.transpose(rk)[0:1, :]
    rows, cols = iotas(n)
    wide = jnp.concatenate([g] * (n // size), axis=1)
    gamma = jnp.where(rows >= cols, jnp.exp(jnp.minimum(wide - g_row, 0.0)), 0.0)
    gamma_rk = gamma * rk_row
    gram = dot(jnp.concatenate([k16, q16], axis=0), k16, 1, 1)
    scale = size**-0.5
    tile = lambda x: jnp.concatenate([x] * (n // size), axis=1)
    a0 = jnp.where(rows > cols, gram[:n] * gamma_rk * tile(rk), 0.0)
    p = gram[n:] * gamma_rk * tile(rq * scale)
    g_end = g[n - 1 : n, :]
    return dict(
        g=g, beta=beta, rk=rk, rq=rq, k_hat=k32 * rk, q_hat=q32 * (rq * scale), gain=jnp.exp(g),
        tail=jnp.exp(g_end - g), gain_end=jnp.exp(g_end), gamma_rk=gamma_rk, a0=a0, p=p,
        rows=rows, cols=cols, tile=tile, scale=scale,
    )


def unit_lower_inverse(a, rows, cols):
    n = a.shape[0]
    differ = rows ^ cols
    eye = (rows == cols).astype(F32)
    x = eye - jnp.where(differ == 1, a, 0.0)
    size = 2
    while size < n:
        part = jnp.where((differ >= size) & (differ < 2 * size), a, 0.0)
        if 2 * size == n:
            x11, x22 = low(x[:size, :size]), low(x[size:, size:])
            x21 = -dot(x22, low(dot(low(a[size:, :size]), x11)))
            top = x[:size]
            bottom = jnp.concatenate([x21, x[size:, size:]], axis=1)
            x = jnp.concatenate([top, bottom], axis=0)
        else:
            x16 = low(x)
            x = x - dot(x16, low(dot(low(part), x16)))
        size *= 2
    ah = low(a)
    al = low(a - ah.astype(F32))
    xh = low(x)
    xl = low(x - xh.astype(F32))
    product = dot(jnp.concatenate([ah, al, ah], axis=1), jnp.concatenate([xh, xh, xl], axis=0))
    return x + dot(xh, low(eye - x - product))


def local_kernel(pack, q_ref, k_ref, do_ref, bp_ref, dp_ref, rate_ref,
                 tg_ref, inv_ref, dr_ref, y_ref, g_ref, b_ref, gt_ref):
    step = pl.program_id(0)

    @pl.when(step == 0)
    def _():
        head_columns(bp_ref[...], dp_ref[...], rate_ref[...], g_ref, b_ref, gt_ref)

    size = q_ref.shape[1] // pack
    for p in range(pack):
        lanes = slice(p * size, (p + 1) * size)
        h = head_common(q_ref[:, lanes], k_ref[:, lanes], step * pack + p, g_ref, b_ref, gt_ref)
        inv = low(unit_lower_inverse(h["a0"] * h["tile"](h["beta"]), h["rows"], h["cols"]))
        inv_ref[p] = inv
        do16 = do_ref[:, lanes]
        d_written = dot(low(h["p"]), do16, 0, 0)
        k_tail = low(h["k_hat"] * h["tail"])
        both = dot(inv, jnp.concatenate([low(d_written), k_tail], axis=1), 0, 0)
        dr16, y16 = low(both[:, :size]), low(both[:, size:])
        dr_ref[:, lanes] = dr16
        y_ref[:, lanes] = y16
        k_in = low(h["k_hat"] * h["beta"] * h["gain"])
        eye = lax.broadcasted_iota(jnp.int32, (size, size), 0) == lax.broadcasted_iota(
            jnp.int32, (size, size), 1
        )
        transition = jnp.where(eye, h["gain_end"], 0.0) - dot(y16, k_in, 0, 0)
        own = dot(
            jnp.concatenate([low(h["q_hat"] * h["gain"]), -k_in], axis=0),
            jnp.concatenate([do16, dr16], axis=0),
            0,
            0,
        )
        tg_ref[0, p] = low(transition)
        tg_ref[1, p] = low(own)


def offset_kernel(pack, y_ref, v_ref, bp_ref, o_ref, b_ref):
    step = pl.program_id(0)

    @pl.when(step == 0)
    def _():
        b_ref[...] = jnp.zeros_like(b_ref)
        b_ref[:, 0 : bp_ref.shape[1]] = 1.0 / (1.0 + jnp.exp(-bp_ref[...]))

    size = y_ref.shape[1] // pack
    for p in range(pack):
        lanes = slice(p * size, (p + 1) * size)
        beta = lane_column(b_ref, step * pack + p)
        o_ref[p] = low(dot(y_ref[:, lanes], low(v_ref[:, lanes].astype(F32) * beta), 0, 0))


def values_kernel(pack, dr_ref, y_ref, e_ref, bp_ref, dv_ref, b_ref):
    step = pl.program_id(0)

    @pl.when(step == 0)
    def _():
        b_ref[...] = jnp.zeros_like(b_ref)
        b_ref[:, 0 : bp_ref.shape[1]] = 1.0 / (1.0 + jnp.exp(-bp_ref[...]))

    size = y_ref.shape[1] // pack
    for p in range(pack):
        lanes = slice(p * size, (p + 1) * size)
        beta = lane_column(b_ref, step * pack + p)
        dr = dr_ref[:, lanes].astype(F32) + dot(y_ref[:, lanes], e_ref[p])
        dv_ref[:, lanes] = low(dr * beta)


def grads_kernel(pack, q_ref, k_ref, v_ref, do_ref, bp_ref, dp_ref, rate_ref, inv_ref, dr_ref, y_ref, s_ref, e_ref,
                 dq_ref, dk_ref, db_ref, dd_ref, g_ref, b_ref, gt_ref, dg_acc, db_acc):
    step = pl.program_id(0)

    @pl.when(step == 0)
    def _():
        head_columns(bp_ref[...], dp_ref[...], rate_ref[...], g_ref, b_ref, gt_ref)
        dg_acc[...] = jnp.zeros_like(dg_acc)
        db_acc[...] = jnp.zeros_like(db_acc)

    size = q_ref.shape[1] // pack
    n = q_ref.shape[0]
    lane = lax.broadcasted_iota(jnp.int32, (n, size), 1)
    row = lax.broadcasted_iota(jnp.int32, (n, size), 0)
    for p in range(pack):
        lanes = slice(p * size, (p + 1) * size)
        head = step * pack + p
        k16, q16, do16 = k_ref[:, lanes], q_ref[:, lanes], do_ref[:, lanes]
        h = head_common(q16, k16, head, g_ref, b_ref, gt_ref)
        beta, rk, k_hat, q_hat, gain, tail = (
            h["beta"], h["rk"], h["k_hat"], h["q_hat"], h["gain"], h["tail"]
        )
        s16, e16 = s_ref[p], e_ref[p]
        inner = v_ref[:, lanes].astype(F32) - gain * (rk * dot(k16, s16))
        written = dot(inv_ref[p], low(beta * inner))
        w16 = low(written)
        dr = dr_ref[:, lanes].astype(F32) + dot(y_ref[:, lanes], e16)
        dr16 = low(dr)
        pair = dot(jnp.concatenate([dr16, do16], axis=0), w16, 1, 1)
        d_a, d_p = -pair[:n], pair[n:]
        weights = d_a * h["a0"] * h["tile"](beta) + d_p * h["p"]
        x1 = low(jnp.where(h["rows"] > h["cols"], d_a * h["gamma_rk"], 0.0))
        x2 = low(d_p * h["gamma_rk"])
        xs = jnp.concatenate([x1, x2], axis=0)
        row_side = dot(xs, k16)
        col_side = dot(xs, jnp.concatenate([low(beta * k_hat), low(q_hat)], axis=0), 0, 0)
        at_s = dot(jnp.concatenate([do16, dr16], axis=0), s16, 1, 1)
        d_qd, dr_s = at_s[:n], at_s[n:]
        d_kt = dot(w16, e16, 1, 1)
        d_q = row_side[n:] + gain * d_qd
        in_term = beta * gain * dr_s
        d_k = rk * (beta * row_side[:n] - in_term + tail * d_kt) + col_side
        unit = q_ref[:, lanes].astype(F32) * h["rq"]
        d_q = h["rq"] * h["scale"] * (d_q - unit * jnp.sum(unit * d_q, axis=1, keepdims=True))
        d_k = d_k - k_hat * jnp.sum(k_hat * d_k, axis=1, keepdims=True)
        dq_ref[:, lanes] = low(d_q)
        dk_ref[:, lanes] = low(d_k)
        tail_term = d_kt * k_hat * tail
        direct = gain * d_qd * q_hat - in_term * k_hat - tail_term
        row_sum = jnp.sum(weights, axis=1, keepdims=True) + jnp.sum(direct, axis=1, keepdims=True)
        col_sum = jnp.sum(weights, axis=0, keepdims=True)
        col_sum = jnp.transpose(jnp.broadcast_to(col_sum, (size, n)))
        end = jnp.sum(tail_term, axis=(0, 1), keepdims=True) + jnp.sum(
            h["gain_end"] * (s16.astype(F32) * e16.astype(F32)), axis=(0, 1), keepdims=True
        )
        dg = row_sum - col_sum + jnp.where(row == n - 1, end, 0.0)
        dg_acc[...] = jnp.where(lane == head, dg, dg_acc[...])
        d_beta = jnp.sum(dr * written, axis=1, keepdims=True)
        db_acc[...] = jnp.where(lane == head, (1.0 - beta) * d_beta, db_acc[...])

    @pl.when(step == pl.num_programs(0) - 1)
    def _():
        heads = bp_ref.shape[1]
        rows, cols = iotas(n)
        d_log = dot((rows <= cols).astype(F32), dg_acc[...], precision=HIGHEST)
        slope = -rate_ref[...] / (1.0 + jnp.exp(-dp_ref[...]))
        dd_ref[...] = d_log[:, 0:heads] * slope
        db_ref[...] = db_acc[:, 0:heads]


def call(body, grid, ins, outs, scratch, name, flops):
    specs = lambda items: [pl.BlockSpec(block, index) for _, block, index in items]
    return pl.pallas_call(
        body,
        grid=(grid,),
        in_specs=specs(ins),
        out_specs=specs(outs),
        out_shape=[a for a, _, _ in outs],
        scratch_shapes=scratch,
        compiler_params=pltpu.CompilerParams(
            dimension_semantics=("arbitrary",), vmem_limit_bytes=VMEM_LIMIT
        ),
        cost_estimate=pl.CostEstimate(flops=flops, bytes_accessed=1 << 20, transcendentals=0),
        name=name,
    )(*[a for a, _, _ in ins])


def shape(dims, dtype):
    return jax.ShapeDtypeStruct(dims, dtype)


def group_total_kernel(group, pos_ref, tg_ref, total_ref):
    pos = pos_ref[0]
    heads = tg_ref.shape[2]
    for i in range(heads):
        slot = pos ^ (group - 1)
        t, g = tg_ref[slot, 0, i].astype(F32), tg_ref[slot, 1, i].astype(F32)
        for j in range(group - 2, -1, -1):
            slot = pos ^ j
            tj = tg_ref[slot, 0, i]
            g = tg_ref[slot, 1, i].astype(F32) + dot(tj, low(g), 0, 0)
            t = dot(low(t), tj)
        total_ref[0, i] = low(t)
        total_ref[1, i] = low(g)


def group_total_forward_kernel(group, pos_ref, tg_ref, o_ref, total_ref):
    pos = pos_ref[0]
    heads = tg_ref.shape[2]
    for i in range(heads):
        t, o = tg_ref[pos, 0, i].astype(F32), o_ref[pos, i].astype(F32)
        for j in range(1, group):
            slot = pos ^ j
            tj = tg_ref[slot, 0, i]
            o = o_ref[slot, i].astype(F32) + dot(tj, low(o))
            t = dot(tj, low(t))
        total_ref[0, i] = low(t)
        total_ref[1, i] = low(o)


def join_kernel(backward, own_ref, far_ref, out_ref):
    for i in range(own_ref.shape[1]):
        near, far = own_ref[0, i], far_ref[0, i]
        if backward:
            out_ref[1, i] = low(own_ref[1, i].astype(F32) + dot(near, far_ref[1, i], 0, 0))
            out_ref[0, i] = low(dot(far, near))
        else:
            out_ref[1, i] = low(own_ref[1, i].astype(F32) + dot(near, far_ref[1, i]))
            out_ref[0, i] = low(dot(near, far))


def spread_back_kernel(group, pos_ref, tg_ref, near_ref, far_ref, out_ref):
    pos = pos_ref[0]
    for i in range(tg_ref.shape[2]):
        e = near_ref[1, i].astype(F32) + dot(near_ref[0, i], far_ref[i], 0, 0)
        for j in range(group - 1, -1, -1):
            slot = pos ^ j
            out_ref[slot, i] = low(e)
            if j:
                e = tg_ref[slot, 1, i].astype(F32) + dot(tg_ref[slot, 0, i], low(e), 0, 0)


def spread_forward_kernel(group, pos_ref, tg_ref, o_ref, near_ref, far_ref, out_ref):
    pos = pos_ref[0]
    for i in range(tg_ref.shape[2]):
        s = near_ref[1, i].astype(F32) + dot(near_ref[0, i], far_ref[i])
        for j in range(group):
            slot = pos ^ j
            out_ref[slot, i] = low(s)
            if j < group - 1:
                s = o_ref[slot, i].astype(F32) + dot(tg_ref[slot, 0, i], low(s))


def small_call(body, name, out_shape, args, flops):
    specs = [
        pl.BlockSpec(memory_space=pltpu.SMEM if a.dtype == jnp.int32 else pltpu.VMEM) for a in args
    ]
    return pl.pallas_call(
        body,
        in_specs=specs,
        out_specs=pl.BlockSpec(memory_space=pltpu.VMEM),
        out_shape=out_shape,
        cost_estimate=pl.CostEstimate(flops=flops, bytes_accessed=1 << 20, transcendentals=0),
        name=name,
    )(*args)


def group_size(count, heads):
    size = 1
    while size * size < count and count % (2 * size) == 0 and heads % (2 * size) == 0:
        size *= 2
    return size


def per_device(queries, keys, hidden, value_weight, beta_pre, decay_pre, decay_rate, out_grad):
    heads = decay_rate.shape[0]
    n, width = queries.shape
    dk = width // heads
    dv = value_weight.shape[1] // heads
    model = hidden.shape[1]
    spans = lax.axis_size("sp")
    group = group_size(spans, heads)
    outer = spans // group
    place = lax.axis_index("sp")
    pos = lax.rem(place, group)
    lead = lax.div(place, group)
    pos_arr = jnp.full((1,), pos, jnp.int32)
    share = heads // group
    pack = 2
    steps = heads // pack
    rate = decay_rate.reshape(1, heads)
    full = lambda a: (a, a.shape, lambda i: (0,) * a.ndim)
    cols = lambda a, w: (a, (n, pack * w), lambda i: (0, i))
    first = lambda a: (a, (pack,) + a.shape[1:], lambda i: (i,) + (0,) * (a.ndim - 1))
    big = heads * n * n * 256

    def near(x, d):
        return lax.ppermute(x, "sp", [(s, s ^ d) for s in range(spans)])

    def along(x, d):
        return lax.ppermute(
            x, "sp", [(s, s + d * group) for s in range(spans) if 0 <= s + d * group < spans]
        )

    rows = model // spans
    by_owner = hidden.reshape(n, outer, group, rows)

    def hidden_part(d):
        return lax.dynamic_index_in_dim(by_owner, pos ^ d, 2, False).reshape(n, outer * rows)

    hidden_parts = [hidden_part(0)] + [near(hidden_part(d), d) for d in range(1, group)]

    tg_shape = shape((2, heads, dk, dk), BF16)
    col_scratch = [pltpu.VMEM((n, 128), F32), pltpu.VMEM((n, 128), F32), pltpu.VMEM((128, n), F32)]
    tg, inv, dr, y = call(
        functools.partial(local_kernel, pack),
        steps,
        [cols(queries, dk), cols(keys, dk), cols(out_grad, dv), full(beta_pre), full(decay_pre), full(rate)],
        [
            (tg_shape, (2, pack, dk, dk), lambda i: (0, i, 0, 0)),
            first(shape((heads, n, n), BF16)),
            cols(shape((n, width), BF16), dv),
            cols(shape((n, width), BF16), dk),
        ],
        col_scratch,
        "local",
        big,
    )

    def to_shares(x, axis):
        parts = []
        for d in range(group):
            piece = lax.dynamic_slice_in_dim(x, (pos ^ d) * share, share, axis)
            parts.append(near(piece, d) if d else piece)
        return jnp.stack(parts)

    def from_shares(x):
        parts = [near(x[d], d) if d else x[d] for d in range(group)]
        ordered = lax.dynamic_update_slice_in_dim
        out = jnp.zeros((heads,) + x.shape[2:], x.dtype)
        for d in range(group):
            out = ordered(out, parts[d], (pos ^ d) * share, 0)
        return out

    small = group * share * dk * dk * dk * 4

    def scan_outer(total, backward):
        sign = -1 if backward else 1
        reach = 1
        inclusive, nearest = total, None
        while True:
            last = 2 * reach >= outer
            if nearest is None:
                nearest = along(inclusive, sign * reach)
                if last:
                    return nearest, jnp.zeros_like(nearest[1])
                inclusive = small_call(
                    functools.partial(join_kernel, backward), "join",
                    shape(total.shape, BF16), [inclusive, nearest], small,
                )
            elif last:
                return nearest, along(inclusive[1], sign * reach)
            else:
                far = along(inclusive, sign * reach)
                join = lambda a, b: small_call(
                    functools.partial(join_kernel, backward), "join",
                    shape(total.shape, BF16), [a, b], small,
                )
                nearest, inclusive = join(nearest, far), join(inclusive, far)
            reach *= 2

    share_shape = shape((2, share, dk, dv), BF16)
    spread_shape = shape((group, share, dk, dv), BF16)

    tg_shared = to_shares(tg, 1)
    back_total = small_call(
        functools.partial(group_total_kernel, group), "total_back", share_shape, [pos_arr, tg_shared], small
    )
    b_near, b_far = scan_outer(back_total, True)
    ends = small_call(
        functools.partial(spread_back_kernel, group), "spread_back", spread_shape,
        [pos_arr, tg_shared, b_near, b_far], small,
    )
    end_grad = from_shares(ends)

    (d_values,) = call(
        functools.partial(values_kernel, pack),
        steps,
        [cols(dr, dv), cols(y, dk), first(end_grad), full(beta_pre)],
        [cols(shape((n, width), BF16), dv)],
        [pltpu.VMEM((n, 128), F32)],
        "values",
        heads * n * dk * dv * 2,
    )
    grad_parts = [d_values] + [near(d_values, d) for d in range(1, group)]
    partial = sum(
        lax.dot_general(a, b, (((0,), (0,)), ((), ())), preferred_element_type=F32)
        for a, b in zip(hidden_parts, grad_parts)
    ).reshape(outer, rows, width)
    d_weight = lax.dynamic_index_in_dim(partial, lead, 0, False)
    for e in range(1, outer):
        target = lax.rem(lead + e, outer)
        piece = lax.dynamic_index_in_dim(partial, target, 0, False).astype(BF16)
        moved = lax.ppermute(
            piece, "sp", [(s, (s + e * group) % spans) for s in range(spans)]
        )
        d_weight = d_weight + moved.astype(F32)

    values = jnp.dot(hidden, value_weight, preferred_element_type=F32).astype(BF16)
    (offset,) = call(
        functools.partial(offset_kernel, pack),
        steps,
        [cols(y, dk), cols(values, dv), full(beta_pre)],
        [first(shape((heads, dk, dv), BF16))],
        [pltpu.VMEM((n, 128), F32)],
        "offset",
        heads * n * dk * dv * 2,
    )
    offset_shared = to_shares(offset, 0)
    forward_total = small_call(
        functools.partial(group_total_forward_kernel, group), "total_forward", share_shape,
        [pos_arr, tg_shared, offset_shared], small,
    )
    f_near, f_far = scan_outer(forward_total, False)
    starts = small_call(
        functools.partial(spread_forward_kernel, group), "spread_forward", spread_shape,
        [pos_arr, tg_shared, offset_shared, f_near, f_far], small,
    )
    start_state = from_shares(starts)

    core = lax.axis_index("tp")
    cores = lax.axis_size("tp")
    own_rows = n // cores

    def input_grad(which):
        piece = lax.dynamic_slice_in_dim(d_values, which * own_rows, own_rows, 0)
        return lax.dot_general(
            piece, value_weight, (((1,), (1,)), ((), ())), preferred_element_type=F32
        )

    d_hidden = input_grad(core)
    for d in range(1, cores):
        moved = lax.ppermute(
            input_grad(lax.rem(core + d, cores)).astype(BF16),
            "tp",
            [(c, (c + d) % cores) for c in range(cores)],
        )
        d_hidden = d_hidden + moved.astype(F32)
    d_hidden = d_hidden.astype(BF16)

    d_queries, d_keys, d_beta, d_decay = call(
        functools.partial(grads_kernel, pack),
        steps,
        [
            cols(queries, dk), cols(keys, dk), cols(values, dv), cols(out_grad, dv), full(beta_pre), full(decay_pre),
            full(rate), first(inv), cols(dr, dv), cols(y, dk), first(start_state), first(end_grad),
        ],
        [
            cols(shape((n, width), BF16), dk),
            cols(shape((n, width), BF16), dk),
            full(shape((n, heads), F32)),
            full(shape((n, heads), F32)),
        ],
        col_scratch + [pltpu.VMEM((n, dk), F32), pltpu.VMEM((n, dk), F32)],
        "grads",
        big,
    )
    return (d_queries, d_keys, d_beta, d_decay, d_hidden, d_weight)


def solution(mesh):
    return jax.shard_map(
        per_device,
        mesh=mesh,
        in_specs=(
            P("sp", "tp"),
            P("sp", "tp"),
            P("sp", None),
            P(None, "tp"),
            P("sp", "tp"),
            P("sp", "tp"),
            P("tp"),
            P("sp", "tp"),
        ),
        out_specs=(
            P("sp", "tp"),
            P("sp", "tp"),
            P("sp", "tp"),
            P("sp", "tp"),
            P(("sp", "tp"), None),
            P("sp", "tp"),
        ),
        check_vma=False,
    )
```

```python
import functools

import jax
import jax.numpy as jnp
from jax import lax
from jax.experimental import pallas as pl
from jax.experimental.pallas import tpu as pltpu
from jax.sharding import PartitionSpec as P

NORM_FLOOR = 16.0
F32 = jnp.float32
BF16 = jnp.bfloat16
HIGHEST = lax.Precision.HIGHEST
VMEM_LIMIT = 56 * 1024 * 1024
PACK = 4
CHUNKS = 2


def dot(a, b, ca=1, cb=0, precision=None):
    return lax.dot_general(
        a, b, (((ca,), (cb,)), ((), ())), precision=precision, preferred_element_type=F32
    )


def low(x):
    return x.astype(BF16)


def iotas(n):
    rows = lax.broadcasted_iota(jnp.int32, (n, n), 0)
    cols = lax.broadcasted_iota(jnp.int32, (n, n), 1)
    return rows, cols


def columns(rows):
    count, n = rows.shape
    return jnp.transpose(jnp.concatenate([rows, jnp.zeros((128 - count, n), F32)], axis=0))


def rate_column(rate_ref):
    count = rate_ref.shape[0]
    row = lax.broadcasted_iota(jnp.int32, (count, 1), 0)
    out = jnp.zeros((count, 1), F32)
    for h in range(count):
        out = jnp.where(row == h, rate_ref[h], out)
    return out


def sigmoid(x):
    return 1.0 / (1.0 + jnp.exp(-x))


def head_columns(beta_ref, decay_ref, rate_ref, g_ref, b_ref, gt_ref):
    decay = decay_ref[...]
    n = decay.shape[1]
    rows, cols = iotas(n)
    log_decay = -rate_column(rate_ref) * (
        jnp.maximum(decay, 0.0) + jnp.log1p(jnp.exp(-jnp.abs(decay)))
    )
    sums = dot(log_decay, (rows <= cols).astype(F32), precision=HIGHEST)
    gt_ref[...] = sums
    g_ref[...] = columns(sums)
    b_ref[...] = columns(sigmoid(beta_ref[...]))


def lane_column(ref, head):
    full = ref[...]
    width = full.shape[1]
    rolled = pltpu.roll(full, lax.rem(width - head, width), 1)
    return jnp.broadcast_to(rolled[:, 0:1], full.shape)


class Head:
    pass


def lanes_of(head, size):
    return pl.ds(pl.multiple_of(head * size, size), size)


def head_common(q_ref, k_ref, head, size, g_ref, b_ref, gt_ref):
    h = Head()
    n = q_ref.shape[0]
    h.head, h.n, h.size = head, n, size
    h.lanes = lanes_of(head, size)
    h.k16, h.q16 = k_ref[:, h.lanes], q_ref[:, h.lanes]
    k32, q32 = h.k16.astype(F32), h.q16.astype(F32)
    h.g = lane_column(g_ref, head)
    h.beta = lane_column(b_ref, head)
    norm = lambda x: jnp.broadcast_to(
        lax.rsqrt(jnp.sum(x * x, axis=1, keepdims=True) + NORM_FLOOR), (n, size)
    )
    h.rk, h.rq = norm(k32), norm(q32)
    g_row = gt_ref[pl.ds(head, 1), :]
    rk_row = jnp.transpose(h.rk)[0:1, :]
    rows, cols = iotas(n)
    h.tile = lambda x: jnp.concatenate([x] * (n // size), axis=1)
    spread = jnp.where(rows >= cols, h.tile(h.g) - g_row, -1e30)
    h.gamma_rk = jnp.exp(spread) * rk_row
    gram = dot(jnp.concatenate([h.k16, h.q16], axis=0), h.k16, 1, 1)
    h.scale = size**-0.5
    h.a0 = jnp.where(rows > cols, gram[:n] * h.gamma_rk * h.tile(h.rk), 0.0)
    h.p = gram[n:] * h.gamma_rk * h.tile(h.rq * h.scale)
    g_end = h.g[n - 1 : n, :]
    h.k_hat, h.q_hat = k32 * h.rk, q32 * (h.rq * h.scale)
    h.gain, h.tail, h.gain_end = jnp.exp(h.g), jnp.exp(g_end - h.g), jnp.exp(g_end)
    return h


def unit_lower_inverses(mats):
    n = mats[0].shape[0]
    rows, cols = iotas(n)
    differ = rows ^ cols
    eye = (rows == cols).astype(F32)
    high = [low(a) for a in mats]
    xs = [low(eye) - a * low((differ == 1).astype(F32)) for a in high]
    size = 2
    while 2 * size < n:
        mask = low(((differ >= size) & (differ < 2 * size)).astype(F32))
        ys = [low(dot(a * mask, x)) for a, x in zip(high, xs)]
        xs = [x - low(dot(x, y)) for x, y in zip(xs, ys)]
        size *= 2
    ys = [low(dot(a[size:, :size], x[:size, :size])) for a, x in zip(high, xs)]
    zs = [low(-dot(x[size:, size:], y)) for x, y in zip(xs, ys)]
    xs = [
        jnp.concatenate([x[:size], jnp.concatenate([z, x[size:, size:]], axis=1)], axis=0)
        for x, z in zip(xs, zs)
    ]
    rest = [low(a - h.astype(F32)) for a, h in zip(mats, high)]
    products = [
        dot(jnp.concatenate([h, l], axis=1), jnp.concatenate([x, x], axis=0))
        for h, l, x in zip(high, rest, xs)
    ]
    return [
        low(x.astype(F32) + dot(x, low(eye - x.astype(F32) - y))) for x, y in zip(xs, products)
    ]


def local_kernel(pack, share, pos_ref, q_ref, k_ref, do_ref, bp_ref, dp_ref, rate_ref, *refs):
    group = q_ref.shape[1] // refs[0].shape[-1] // share
    tg_refs, (inv_ref, dr_ref, y_ref, g_ref, b_ref, gt_ref) = refs[:group], refs[group:]
    pos = pos_ref[0]
    head_columns(bp_ref, dp_ref, rate_ref, g_ref, b_ref, gt_ref)
    size = tg_refs[0].shape[-1]
    for start in range(0, group * share, pack):
        places = range(start, start + pack)
        heads = [
            head_common(q_ref, k_ref, ((p // share) ^ pos) * share + p % share, size, g_ref, b_ref, gt_ref)
            for p in places
        ]
        invs = unit_lower_inverses([h.a0 * h.tile(h.beta) for h in heads])
        outs = [do_ref[:, h.lanes] for h in heads]
        d_written = [low(dot(low(h.p), do16, 0, 0)) for h, do16 in zip(heads, outs)]
        tails = [low(h.k_hat * h.tail) for h in heads]
        both = [
            low(dot(inv, jnp.concatenate([d, t], axis=1), 0, 0))
            for inv, d, t in zip(invs, d_written, tails)
        ]
        eye = lax.broadcasted_iota(jnp.int32, (size, size), 0) == lax.broadcasted_iota(
            jnp.int32, (size, size), 1
        )
        for p, h, inv, do16, b16 in zip(places, heads, invs, outs, both):
            dr16, y16 = b16[:, :size], b16[:, size:]
            inv_ref[p] = inv
            dr_ref[:, h.lanes] = dr16
            y_ref[:, h.lanes] = y16
            k_in = low(h.k_hat * h.beta * h.gain)
            out = tg_refs[p // share]
            out[0, p % share] = low(jnp.where(eye, h.gain_end, 0.0) - dot(y16, k_in, 0, 0))
            own = dot(
                jnp.concatenate([low(h.q_hat * h.gain), -k_in], axis=0),
                jnp.concatenate([do16, dr16], axis=0), 0, 0,
            )
            out[1, p % share] = low(own)


def offset_kernel(share, pos_ref, y_ref, v_ref, bp_ref, *refs):
    o_refs, b_ref = refs[:-1], refs[-1]
    pos = pos_ref[0]
    b_ref[...] = columns(sigmoid(bp_ref[...]))
    size = o_refs[0].shape[-1]
    for p in range(len(o_refs) * share):
        head = ((p // share) ^ pos) * share + p % share
        lanes = lanes_of(head, size)
        beta = lane_column(b_ref, head)
        o_refs[p // share][p % share] = low(
            dot(y_ref[:, lanes], low(v_ref[:, lanes].astype(F32) * beta), 0, 0)
        )


def values_kernel(share, pos_ref, dr_ref, y_ref, bp_ref, *refs):
    e_refs, (dv_ref, b_ref) = refs[:-2], refs[-2:]
    pos = pos_ref[0]
    b_ref[...] = columns(sigmoid(bp_ref[...]))
    size = e_refs[0].shape[-1]
    for p in range(len(e_refs) * share):
        head = ((p // share) ^ pos) * share + p % share
        lanes = lanes_of(head, size)
        beta = lane_column(b_ref, head)
        dr = dr_ref[:, lanes].astype(F32) + dot(y_ref[:, lanes], e_refs[p // share][p % share])
        dv_ref[:, lanes] = low(dr * beta)


def grads_kernel(pack, share, pos_ref, q_ref, k_ref, v_ref, do_ref, bp_ref, dp_ref, rate_ref, inv_ref, dr_ref, y_ref, *refs):
    size = refs[0].shape[-1]
    group = q_ref.shape[1] // size // share
    s_refs, e_refs = refs[:group], refs[group : 2 * group]
    dq_ref, dk_ref, db_ref, dd_ref, g_ref, b_ref, gt_ref, row_acc, col_acc, db_acc = refs[2 * group :]
    pos = pos_ref[0]
    head_columns(bp_ref, dp_ref, rate_ref, g_ref, b_ref, gt_ref)
    count = group * share
    n = q_ref.shape[0]
    rows, cols = iotas(n)
    lane = lax.broadcasted_iota(jnp.int32, (n, size), 1)
    row_acc[...] = jnp.zeros_like(row_acc)
    db_acc[...] = jnp.zeros_like(db_acc)
    for start in range(0, count, pack):
        places = range(start, start + pack)
        heads = [
            head_common(q_ref, k_ref, ((p // share) ^ pos) * share + p % share, size, g_ref, b_ref, gt_ref)
            for p in places
        ]
        for p, h in zip(places, heads):
            h.s16, h.e16 = s_refs[p // share][p % share], e_refs[p // share][p % share]
            h.do16 = do_ref[:, h.lanes]
            inner = v_ref[:, h.lanes].astype(F32) - h.gain * (h.rk * dot(h.k16, h.s16))
            h.right = low(h.beta * inner)
            h.dr = dr_ref[:, h.lanes].astype(F32) + dot(y_ref[:, h.lanes], h.e16)
            h.dr16 = low(h.dr)
        for p, h in zip(places, heads):
            h.written = dot(inv_ref[p], h.right)
            h.w16 = low(h.written)
            at_s = dot(jnp.concatenate([h.do16, h.dr16], axis=0), h.s16, 1, 1)
            h.d_qd, h.dr_s = at_s[:n], at_s[n:]
        for h in heads:
            pair = dot(jnp.concatenate([-h.dr16, h.do16], axis=0), h.w16, 1, 1)
            d_a, d_p = pair[:n], pair[n:]
            h.weights = d_a * h.a0 * h.tile(h.beta) + d_p * h.p
            x1 = low(jnp.where(rows > cols, d_a * h.gamma_rk, 0.0))
            x2 = low(d_p * h.gamma_rk)
            h.xs = jnp.concatenate([x1, x2], axis=0)
            h.d_kt = dot(h.w16, h.e16, 1, 1)
        for h in heads:
            row_side = dot(h.xs, h.k16)
            col_side = dot(
                h.xs, jnp.concatenate([low(h.beta * h.k_hat), low(h.q_hat)], axis=0), 0, 0
            )
            d_q = row_side[n:] + h.gain * h.d_qd
            in_term = h.beta * h.gain * h.dr_s
            d_k = h.rk * (h.beta * row_side[:n] - in_term + h.tail * h.d_kt) + col_side
            unit = h.q16.astype(F32) * h.rq
            d_q = h.rq * h.scale * (d_q - unit * jnp.sum(unit * d_q, axis=1, keepdims=True))
            d_k = d_k - h.k_hat * jnp.sum(h.k_hat * d_k, axis=1, keepdims=True)
            dq_ref[:, h.lanes] = low(d_q)
            dk_ref[:, h.lanes] = low(d_k)
            tail_term = h.d_kt * h.k_hat * h.tail
            direct = h.gain * h.d_qd * h.q_hat - in_term * h.k_hat - tail_term
            folded = sum(h.weights[:, i * size : (i + 1) * size] for i in range(n // size))
            row_sum = jnp.sum(folded + direct, axis=1, keepdims=True)
            end = jnp.sum(
                jnp.sum(tail_term, axis=0, keepdims=True)
                + jnp.sum(h.gain_end * (h.s16.astype(F32) * h.e16.astype(F32)), axis=0, keepdims=True),
                axis=1, keepdims=True,
            )
            last = lax.broadcasted_iota(jnp.int32, (1, n), 1) == n - 1
            col_acc[pl.ds(h.head, 1), :] = jnp.where(last, end, 0.0) - jnp.sum(
                h.weights, axis=0, keepdims=True
            )
            row_acc[...] = jnp.where(lane == h.head, row_sum, row_acc[...])
            d_beta = (1.0 - h.beta) * jnp.sum(h.dr * h.written, axis=1, keepdims=True)
            db_acc[...] = jnp.where(lane == h.head, d_beta, db_acc[...])
    d_sums = jnp.transpose(row_acc[...])[0:count] + col_acc[...]
    d_log = dot(d_sums, (rows >= cols).astype(F32), precision=HIGHEST)
    dd_ref[...] = -rate_column(rate_ref) * sigmoid(dp_ref[...]) * d_log
    db_ref[...] = jnp.transpose(db_acc[...])[0:count]


def call(body, name, args, outs, scratch=(), flops=0):
    place = lambda a: pl.BlockSpec(memory_space=pltpu.SMEM if a.ndim == 1 else pltpu.VMEM)
    return pl.pallas_call(
        body,
        in_specs=[place(a) for a in args],
        out_specs=[pl.BlockSpec(memory_space=pltpu.VMEM) for _ in outs],
        out_shape=outs,
        scratch_shapes=list(scratch),
        compiler_params=pltpu.CompilerParams(vmem_limit_bytes=VMEM_LIMIT),
        cost_estimate=pl.CostEstimate(flops=flops, bytes_accessed=1 << 20, transcendentals=0),
        name=name,
    )(*args)


def shape(*dims, dtype=BF16):
    return jax.ShapeDtypeStruct(dims, dtype)


def total_kernel(group, backward, pos_ref, *refs):
    count = len(refs) - 2
    tg_refs, o_refs, (total_ref, store) = refs[:group], refs[group:count], refs[count:]
    pos = pos_ref[0]
    share = total_ref.shape[1]
    for d in range(group):
        store[d, 0] = tg_refs[d][0]
        store[d, 1] = tg_refs[d][1] if backward else o_refs[d][...]
    order = list(range(group))
    if backward:
        order.reverse()
    for i in range(share):
        first = pos ^ order[0]
        t, o = store[first, 0, i], store[first, 1, i]
        for j in order[1:]:
            slot = pos ^ j
            tj, oj = store[slot, 0, i], store[slot, 1, i].astype(F32)
            if backward:
                o, t = low(oj + dot(tj, o, 0, 0)), low(dot(t, tj))
            else:
                o, t = low(oj + dot(tj, o)), low(dot(tj, t))
        total_ref[0, i] = t
        total_ref[1, i] = o


def spread_kernel(group, outer, backward, pos_ref, *refs):
    reach = outer - 1
    tg_refs, refs = refs[:group], refs[group:]
    o_refs, refs = (None, refs) if backward else (refs[:group], refs[group:])
    far_refs, out_refs, store, result = refs[:reach], refs[reach : reach + group], refs[-2], refs[-1]
    pos = pos_ref[0]
    share = out_refs[0].shape[0]
    for d in range(group):
        store[d, 0] = tg_refs[d][0]
        store[d, 1] = tg_refs[d][1] if backward else o_refs[d][...]
    turn = (lambda t, x: dot(t, x, 0, 0)) if backward else (lambda t, x: dot(t, x))
    state = [jnp.zeros(store.shape[3:], BF16)] * share
    for far in reversed(far_refs):
        if far is far_refs[-1]:
            state = [far[far.shape[0] - 1, i] for i in range(share)]
        else:
            state = [low(far[1, i].astype(F32) + turn(far[0, i], x)) for i, x in enumerate(state)]
    order = list(range(group))
    if backward:
        order.reverse()
    for j in order:
        slot = pos ^ j
        for i in range(share):
            result[slot, i] = state[i]
        if j != order[-1]:
            state = [
                low(store[slot, 1, i].astype(F32) + turn(store[slot, 0, i], x))
                for i, x in enumerate(state)
            ]
    for d in range(group):
        out_refs[d][...] = result[d]


def group_size(count, heads):
    size = 1
    while size * size < count and count % (2 * size) == 0 and heads % (2 * size) == 0:
        size *= 2
    return size


def per_device(queries, keys, hidden, value_weight, beta_pre, decay_pre, decay_rate, out_grad):
    heads = decay_rate.shape[0]
    n, width = queries.shape
    dk = width // heads
    dv = value_weight.shape[1] // heads
    model = hidden.shape[1]
    spans = lax.axis_size("sp")
    group = group_size(spans, heads)
    outer = spans // group
    place = lax.axis_index("sp")
    pos = lax.rem(place, group)
    lead = lax.div(place, group)
    pos_arr = jnp.full((1,), pos, jnp.int32)
    share = heads // group
    beta_t, decay_t = beta_pre.T, decay_pre.T
    big = heads * n * n * 256

    def near(x, d):
        return lax.ppermute(x, "sp", [(s, s ^ d) for s in range(spans)]) if d else x

    def along(x, d):
        return lax.ppermute(
            x, "sp", [(s, s + d * group) for s in range(spans) if 0 <= s + d * group < spans]
        )

    def tied(x, after):
        return lax.optimization_barrier((x, after))[0]

    rows = model // spans
    by_owner = hidden.reshape(n, outer, group, rows)

    def hidden_part(d):
        return lax.dynamic_index_in_dim(by_owner, pos ^ d, 2, False).reshape(n, outer * rows)

    hidden_parts = [near(hidden_part(d), d) for d in range(group)]

    col_scratch = [
        pltpu.VMEM((n, 128), F32), pltpu.VMEM((n, 128), F32), pltpu.VMEM((heads, n), F32)
    ]
    *tg, inv, dr, y = call(
        functools.partial(local_kernel, PACK, share),
        "local",
        [pos_arr, queries, keys, out_grad, beta_t, decay_t, decay_rate],
        [shape(2, share, dk, dv)] * group + [shape(heads, n, n), shape(n, width), shape(n, width)],
        col_scratch,
        big,
    )
    small = group * share * dk * dk * dk * 4
    store = pltpu.VMEM((group, 2, share, dk, dv), BF16)
    result = pltpu.VMEM((group, share, dk, dv), BF16)

    def states(backward, maps, offsets):
        name = "back" if backward else "forward"
        (total,) = call(
            functools.partial(total_kernel, group, backward), "total_" + name,
            [pos_arr, *maps, *offsets], [shape(2, share, dk, dv)], [store], small,
        )
        sign = -1 if backward else 1
        far = [
            along(total if d < outer - 1 else total[1:], sign * d) for d in range(1, outer)
        ]
        spread = call(
            functools.partial(spread_kernel, group, outer, backward), "spread_" + name,
            [pos_arr, *maps, *offsets, *far], [shape(share, dk, dv)] * group, [store, result], small,
        )
        return [near(x, d) for d, x in enumerate(spread)], total, far

    tg = [near(x, d) for d, x in enumerate(tg)]
    end_grad, back_total, back_far = states(True, tg, [])

    (d_values,) = call(
        functools.partial(values_kernel, share),
        "values",
        [pos_arr, dr, y, beta_t, *end_grad],
        [shape(n, width)],
        [pltpu.VMEM((n, 128), F32)],
        heads * n * dk * dv * 2,
    )
    chunk = width // CHUNKS
    pieces = []
    for c in range(CHUNKS):
        own = lax.slice_in_dim(d_values, c * chunk, (c + 1) * chunk, axis=1)
        partial = sum(
            lax.dot_general(a, near(own, d), (((0,), (0,)), ((), ())), preferred_element_type=F32)
            for d, a in enumerate(hidden_parts)
        ).reshape(outer, rows, chunk)
        total = lax.dynamic_index_in_dim(partial, lead, 0, False)
        for e in range(1, outer):
            piece = lax.dynamic_index_in_dim(partial, lax.rem(lead + e, outer), 0, False)
            moved = lax.ppermute(
                piece.astype(BF16), "sp", [(s, (s + e * group) % spans) for s in range(spans)]
            )
            total = total + moved.astype(F32)
        pieces.append(total)
    d_weight = jnp.concatenate(pieces, axis=1)

    values = jnp.dot(hidden, value_weight, preferred_element_type=F32).astype(BF16)
    offset = call(
        functools.partial(offset_kernel, share),
        "offset",
        [pos_arr, y, values, beta_t],
        [shape(share, dk, dv)] * group,
        [pltpu.VMEM((n, 128), F32)],
        heads * n * dk * dv * 2,
    )
    offset = tied(offset, back_total)
    offset = [near(x, d) for d, x in enumerate(offset)]
    start_state, _, _ = states(False, tg, offset)

    core = lax.axis_index("tp")
    cores = lax.axis_size("tp")
    own_rows = n // cores

    def input_grad(which):
        piece = lax.dynamic_slice_in_dim(d_values, which * own_rows, own_rows, 0)
        return lax.dot_general(
            piece, value_weight, (((1,), (1,)), ((), ())), preferred_element_type=F32
        )

    d_hidden = input_grad(core)
    for d in range(1, cores):
        moved = lax.ppermute(
            input_grad(lax.rem(core + d, cores)).astype(BF16),
            "tp",
            [(c, (c + d) % cores) for c in range(cores)],
        )
        d_hidden = d_hidden + moved.astype(F32)
    d_hidden = d_hidden.astype(BF16)

    d_queries, d_keys, d_beta, d_decay = call(
        functools.partial(grads_kernel, PACK, share),
        "grads",
        [pos_arr, queries, keys, values, out_grad, beta_t, decay_t, decay_rate, inv, dr, y, *start_state, *end_grad],
        [shape(n, width), shape(n, width), shape(heads, n, dtype=F32), shape(heads, n, dtype=F32)],
        col_scratch + [pltpu.VMEM((n, dk), F32), pltpu.VMEM((heads, n), F32), pltpu.VMEM((n, dk), F32)],
        big,
    )
    return (d_queries, d_keys, d_beta.T, d_decay.T, d_hidden, d_weight)


def solution(mesh):
    return jax.shard_map(
        per_device,
        mesh=mesh,
        in_specs=(
            P("sp", "tp"),
            P("sp", "tp"),
            P("sp", None),
            P(None, "tp"),
            P("sp", "tp"),
            P("sp", "tp"),
            P("tp"),
            P("sp", "tp"),
        ),
        out_specs=(
            P("sp", "tp"),
            P("sp", "tp"),
            P("sp", "tp"),
            P("sp", "tp"),
            P(("sp", "tp"), None),
            P("sp", "tp"),
        ),
        check_vma=False,
    )
```

```python
import functools

import jax
import jax.numpy as jnp
from jax import lax
from jax.experimental import pallas as pl
from jax.experimental.pallas import tpu as pltpu
from jax.sharding import PartitionSpec as P


NORM_FLOOR = 16.0
F32 = jnp.float32
BF16 = jnp.bfloat16
HIGHEST = lax.Precision.HIGHEST
VMEM_LIMIT = 56 * 1024 * 1024
PACK = 8
CHUNKS = 2


def dot(a, b, ca=1, cb=0, precision=None):
    return lax.dot_general(
        a, b, (((ca,), (cb,)), ((), ())), precision=precision, preferred_element_type=F32
    )


def low(x):
    return x.astype(BF16)


def iotas(n):
    rows = lax.broadcasted_iota(jnp.int32, (n, n), 0)
    cols = lax.broadcasted_iota(jnp.int32, (n, n), 1)
    return rows, cols


def columns(rows):
    count, n = rows.shape
    return jnp.transpose(jnp.concatenate([rows, jnp.zeros((128 - count, n), F32)], axis=0))


def rate_column(rate_ref):
    count = rate_ref.shape[0]
    row = lax.broadcasted_iota(jnp.int32, (count, 1), 0)
    out = jnp.zeros((count, 1), F32)
    for h in range(count):
        out = jnp.where(row == h, rate_ref[h], out)
    return out


def sigmoid(x):
    return 1.0 / (1.0 + jnp.exp(-x))


def head_columns(beta_ref, decay_ref, rate_ref, g_ref, b_ref, gt_ref):
    decay = decay_ref[...]
    n = decay.shape[1]
    rows, cols = iotas(n)
    log_decay = -rate_column(rate_ref) * (
        jnp.maximum(decay, 0.0) + jnp.log1p(jnp.exp(-jnp.abs(decay)))
    )
    sums = dot(log_decay, (rows <= cols).astype(F32), precision=HIGHEST)
    gt_ref[...] = sums
    g_ref[...] = columns(sums)
    b_ref[...] = columns(sigmoid(beta_ref[...]))


def lane_column(ref, head):
    return jnp.broadcast_to(ref[:, head : head + 1], ref.shape)


class Head:
    pass


def lanes_of(head, size):
    return slice(head * size, (head + 1) * size)


def head_common(q_ref, k_ref, head, size, g_ref, b_ref, gt_ref):
    h = Head()
    n = q_ref.shape[0]
    h.head, h.n, h.size = head, n, size
    h.lanes = lanes_of(head, size)
    h.k16, h.q16 = k_ref[:, h.lanes], q_ref[:, h.lanes]
    k32, q32 = h.k16.astype(F32), h.q16.astype(F32)
    h.g = lane_column(g_ref, head)
    h.beta = lane_column(b_ref, head)
    norm = lambda x: jnp.broadcast_to(
        lax.rsqrt(jnp.sum(x * x, axis=1, keepdims=True) + NORM_FLOOR), (n, size)
    )
    h.rk, h.rq = norm(k32), norm(q32)
    g_row = gt_ref[head : head + 1, :]
    rk_row = jnp.transpose(h.rk)[0:1, :]
    rows, cols = iotas(n)
    h.tile = lambda x: jnp.concatenate([x] * (n // size), axis=1)
    spread = jnp.where(rows >= cols, h.tile(h.g) - g_row, -1e30)
    h.gamma_rk = jnp.exp(spread) * rk_row
    gram = dot(jnp.concatenate([h.k16, h.q16], axis=0), h.k16, 1, 1)
    h.scale = size**-0.5
    h.a0 = jnp.where(rows > cols, gram[:n] * h.gamma_rk * h.tile(h.rk), 0.0)
    h.p = gram[n:] * h.gamma_rk * h.tile(h.rq * h.scale)
    g_end = h.g[n - 1 : n, :]
    h.k_hat, h.q_hat = k32 * h.rk, q32 * (h.rq * h.scale)
    h.gain, h.tail, h.gain_end = jnp.exp(h.g), jnp.exp(g_end - h.g), jnp.exp(g_end)
    return h


def unit_lower_inverses(mats):
    n = mats[0].shape[0]
    rows, cols = iotas(n)
    differ = rows ^ cols
    eye = (rows == cols).astype(F32)
    high = [low(a) for a in mats]
    xs = [low(eye) - a * low((differ == 1).astype(F32)) for a in high]
    size = 2
    while 2 * size < n:
        mask = low(((differ >= size) & (differ < 2 * size)).astype(F32))
        ys = [low(dot(a * mask, x)) for a, x in zip(high, xs)]
        xs = [x - low(dot(x, y)) for x, y in zip(xs, ys)]
        size *= 2
    ys = [low(dot(a[size:, :size], x[:size, :size])) for a, x in zip(high, xs)]
    zs = [low(-dot(x[size:, size:], y)) for x, y in zip(xs, ys)]
    xs = [
        jnp.concatenate([x[:size], jnp.concatenate([z, x[size:, size:]], axis=1)], axis=0)
        for x, z in zip(xs, zs)
    ]
    rest = [low(a - h.astype(F32)) for a, h in zip(mats, high)]
    products = [
        dot(jnp.concatenate([h, l], axis=1), jnp.concatenate([x, x], axis=0))
        for h, l, x in zip(high, rest, xs)
    ]
    return [
        low(x.astype(F32) + dot(x, low(eye - x.astype(F32) - y))) for x, y in zip(xs, products)
    ]


def local_kernel(pack, share, outer, pos_ref, q_ref, k_ref, do_ref, hid_ref, w_ref, bp_ref, dp_ref, rate_ref, maps,
                 *refs):
    inv_ref, dr_ref, y_ref, bdr_ref, by_ref, v_ref, g_ref, b_ref, gt_ref, hid, hid_t, w, sems = refs[: 6] + refs[6 + maps.shape[0] :]
    hid_parts = refs[6 : 6 + maps.shape[0]]
    copies = [
        pltpu.make_async_copy(hid_ref, hid, sems.at[0]),
        pltpu.make_async_copy(w_ref, w, sems.at[1]),
    ]
    for copy in copies:
        copy.start()
    head_columns(bp_ref, dp_ref, rate_ref, g_ref, b_ref, gt_ref)
    size = maps.shape[-1]
    for start in range(0, maps.shape[0] * share, pack):
        places = range(start, start + pack)
        heads = [head_common(q_ref, k_ref, p, size, g_ref, b_ref, gt_ref) for p in places]
        outs = [do_ref[:, h.lanes] for h in heads]
        d_written = [low(dot(low(h.p), do16, 0, 0)) for h, do16 in zip(heads, outs)]
        invs = unit_lower_inverses([h.a0 * h.tile(h.beta) for h in heads])
        tails = [low(h.k_hat * h.tail) for h in heads]
        both = [
            dot(inv, jnp.concatenate([d, t], axis=1), 0, 0)
            for inv, d, t in zip(invs, d_written, tails)
        ]
        if start == 0:
            for copy in copies:
                copy.wait()
            v_ref[...] = low(dot(hid[...], w[...]))
            rows = hid.shape[1] // outer // maps.shape[0]
            hid_t[...] = jnp.transpose(hid[...])
            for d, part in enumerate(hid_parts):
                for e in range(outer):
                    at = pl.multiple_of((e * maps.shape[0] + (pos_ref[0] ^ d)) * rows, rows)
                    part[e * rows : (e + 1) * rows, :] = hid_t[pl.ds(at, rows), :]
        eye = lax.broadcasted_iota(jnp.int32, (size, size), 0) == lax.broadcasted_iota(
            jnp.int32, (size, size), 1
        )
        for p, h, inv, do16, b32 in zip(places, heads, invs, outs, both):
            dr16, y16 = low(b32[:, :size]), low(b32[:, size:])
            inv_ref[p] = inv
            dr_ref[:, h.lanes] = dr16
            y_ref[:, h.lanes] = y16
            bdr_ref[:, h.lanes] = low(h.beta * b32[:, :size])
            by_ref[:, h.lanes] = low(h.beta * b32[:, size:])
            k_in = low(h.k_hat * h.beta * h.gain)
            value = low(h.beta * v_ref[:, h.lanes].astype(F32))
            out = maps.at[p // share]
            into = dot(y16, jnp.concatenate([k_in, value], axis=1), 0, 0)
            out[0, p % share] = low(jnp.where(eye, h.gain_end, 0.0) - into[:, :size])
            own = dot(
                jnp.concatenate([do16, dr16], axis=0),
                jnp.concatenate([low(h.q_hat * h.gain), -k_in], axis=0), 0, 0,
            )
            out[1, p % share] = low(own)
            out[2, p % share] = low(into[:, size:])


def values_kernel(share, chunks, bdr_ref, by_ref, states, dv_ref, *parts):
    size = states.shape[-1]
    count = states.shape[0] * share
    per = count // chunks
    for h in range(count):
        lanes = slice(h * size, (h + 1) * size)
        dv = low(bdr_ref[:, lanes].astype(F32) + dot(by_ref[:, lanes], states[h // share, 0, h % share], 1, 1))
        dv_ref[:, lanes] = dv
        parts[h // per][:, (h % per) * size : (h % per + 1) * size] = dv


def weight_kernel(group, outer, lead_ref, *refs):
    hid_refs, grad_refs, out_refs, store = refs[:group], refs[group : 2 * group], refs[2 * group : -1], refs[-1]
    rows = store.shape[0] // outer
    store[...] = dot(
        jnp.concatenate([r[...] for r in hid_refs], axis=1),
        jnp.concatenate([r[...] for r in grad_refs], axis=0),
    )
    lead = lead_ref[0]
    for e in range(outer):
        block = store[pl.ds(pl.multiple_of(lax.rem(lead + e, outer) * rows, rows), rows), :]
        out_refs[e][...] = block.astype(out_refs[e].dtype)


def input_kernel(cores, core_ref, dv_ref, w_ref, *refs):
    out_refs, store = refs[:-1], refs[-1]
    rows = dv_ref.shape[0] // cores
    core = core_ref[0]
    store[...] = dot(dv_ref[...], w_ref[...], 1, 1)
    for d, out_ref in enumerate(out_refs):
        start = pl.multiple_of(lax.rem(core + d, cores) * rows, rows)
        out_ref[...] = store[pl.ds(start, rows), :].astype(out_ref.dtype)


def add_kernel(*refs):
    refs[-1][...] = low(sum(r[...].astype(F32) for r in refs[:-1]))


def sum_kernel(outer, *refs):
    out_ref = refs[-1]
    chunks = (len(refs) - 1) // outer
    width = refs[0].shape[1]
    for c in range(chunks):
        parts = refs[c * outer : (c + 1) * outer]
        out_ref[:, c * width : (c + 1) * width] = sum(r[...].astype(F32) for r in parts)


def grads_kernel(pack, share, q_ref, k_ref, v_ref, do_ref, bp_ref, dp_ref, rate_ref, inv_ref, dr_ref, y_ref, states,
                 dq_ref, dk_ref, db_ref, dd_ref, g_ref, b_ref, gt_ref, row_acc, col_acc, db_acc):
    size = states.shape[-1]
    head_columns(bp_ref, dp_ref, rate_ref, g_ref, b_ref, gt_ref)
    count = states.shape[0] * share
    n = q_ref.shape[0]
    rows, cols = iotas(n)
    lane = lax.broadcasted_iota(jnp.int32, (n, size), 1)
    row_acc[...] = jnp.zeros_like(row_acc)
    db_acc[...] = jnp.zeros_like(db_acc)
    for start in range(0, count, pack):
        places = range(start, start + pack)
        heads = [head_common(q_ref, k_ref, p, size, g_ref, b_ref, gt_ref) for p in places]
        for p, h in zip(places, heads):
            h.e16, h.s16 = states[p // share, 0, p % share], states[p // share, 1, p % share]
            h.do16 = do_ref[:, h.lanes]
            inner = v_ref[:, h.lanes].astype(F32) - h.gain * (h.rk * dot(h.k16, h.s16))
            h.right = low(h.beta * inner)
            h.dr = dr_ref[:, h.lanes].astype(F32) + dot(y_ref[:, h.lanes], h.e16, 1, 1)
            h.dr16 = low(h.dr)
        for p, h in zip(places, heads):
            h.written = dot(inv_ref[p], h.right)
            h.w16 = low(h.written)
            at_s = dot(jnp.concatenate([h.do16, h.dr16], axis=0), h.s16, 1, 1)
            h.d_qd, h.dr_s = at_s[:n], at_s[n:]
        for h in heads:
            pair = dot(jnp.concatenate([-h.dr16, h.do16], axis=0), h.w16, 1, 1)
            d_a, d_p = pair[:n], pair[n:]
            h.weights = d_a * h.a0 * h.tile(h.beta) + d_p * h.p
            x1 = low(jnp.where(rows > cols, d_a * h.gamma_rk, 0.0))
            x2 = low(d_p * h.gamma_rk)
            h.xs = jnp.concatenate([x1, x2], axis=0)
            h.d_kt = dot(h.w16, h.e16)
        for h in heads:
            row_side = dot(h.xs, h.k16)
            col_side = dot(
                h.xs, jnp.concatenate([low(h.beta * h.k_hat), low(h.q_hat)], axis=0), 0, 0
            )
            d_q = row_side[n:] + h.gain * h.d_qd
            in_term = h.beta * h.gain * h.dr_s
            d_k = h.rk * (h.beta * row_side[:n] - in_term + h.tail * h.d_kt) + col_side
            unit = h.q16.astype(F32) * h.rq
            d_q = h.rq * h.scale * (d_q - unit * jnp.sum(unit * d_q, axis=1, keepdims=True))
            d_k = d_k - h.k_hat * jnp.sum(h.k_hat * d_k, axis=1, keepdims=True)
            dq_ref[:, h.lanes] = low(d_q)
            dk_ref[:, h.lanes] = low(d_k)
            tail_term = h.d_kt * h.k_hat * h.tail
            direct = h.gain * h.d_qd * h.q_hat - in_term * h.k_hat - tail_term
            folded = sum(h.weights[:, i * size : (i + 1) * size] for i in range(n // size))
            row_sum = jnp.sum(folded + direct, axis=1, keepdims=True)
            end = jnp.sum(
                jnp.sum(tail_term, axis=0, keepdims=True)
                + jnp.sum(h.gain_end * (h.s16.astype(F32) * jnp.transpose(h.e16.astype(F32))), axis=0, keepdims=True),
                axis=1, keepdims=True,
            )
            last = lax.broadcasted_iota(jnp.int32, (1, n), 1) == n - 1
            col_acc[h.head : h.head + 1, :] = jnp.where(last, end, 0.0) - jnp.sum(
                h.weights, axis=0, keepdims=True
            )
            row_acc[...] = jnp.where(lane == h.head, row_sum, row_acc[...])
            d_beta = (1.0 - h.beta) * jnp.sum(h.dr * h.written, axis=1, keepdims=True)
            db_acc[...] = jnp.where(lane == h.head, d_beta, db_acc[...])
    d_sums = jnp.transpose(row_acc[...])[0:count] + col_acc[...]
    d_log = dot(d_sums, (rows >= cols).astype(F32), precision=HIGHEST)
    dd_ref[...] = -rate_column(rate_ref) * sigmoid(dp_ref[...]) * d_log
    db_ref[...] = jnp.transpose(db_acc[...])[0:count]


def call(body, args, outs, scratch=(), flops=0, anywhere=()):
    def place(i, a):
        space = pltpu.SMEM if a.ndim == 1 else pl.ANY if i in anywhere else pltpu.VMEM
        return pl.BlockSpec(memory_space=space)

    return pl.pallas_call(
        body,
        in_specs=[place(i, a) for i, a in enumerate(args)],
        out_specs=[pl.BlockSpec(memory_space=pltpu.VMEM) for _ in outs],
        out_shape=outs,
        scratch_shapes=list(scratch),
        compiler_params=pltpu.CompilerParams(vmem_limit_bytes=VMEM_LIMIT),
        cost_estimate=pl.CostEstimate(flops=flops, bytes_accessed=1 << 20, transcendentals=0),
    )(*args)


def shape(*dims, dtype=BF16):
    return jax.ShapeDtypeStruct(dims, dtype)


def total_kernel(maps, total_ref):
    group, _, share = maps.shape[:3]
    for i in range(share):
        g, o, t = maps[group - 1, 1, i], maps[0, 2, i], maps[0, 0, i]
        for j in range(1, group):
            b = group - 1 - j
            g = low(maps[b, 1, i].astype(F32) + dot(g, maps[b, 0, i]))
            o = low(maps[j, 2, i].astype(F32) + dot(maps[j, 0, i], o))
            t = low(dot(maps[j, 0, i], t))
        total_ref[0, i], total_ref[1, i], total_ref[2, i] = t, g, o


def join_kernel(level, last, lead_ref, own, other, out_ref, both):
    lead = lead_ref[0]
    bit = (lead >> level) & 1
    both[bit] = own[...]
    both[1 - bit] = other[...]
    for i in range(own.shape[1]):
        g = low(both[0, 1, i].astype(F32) + dot(both[1, 1, i], both[0, 0, i]))
        o = low(both[1, 2, i].astype(F32) + dot(both[1, 0, i], both[0, 2, i]))
        if last:
            out_ref[i] = jnp.where((lead >> (level + 1)) & 1 == 0, o, g)
        else:
            out_ref[0, i], out_ref[1, i], out_ref[2, i] = low(dot(both[1, 0, i], both[0, 0, i])), g, o


def spread_kernel(levels, lead_ref, maps, *refs):
    ranges, far, result = refs[: 2 * levels], refs[2 * levels], refs[2 * levels + 1]
    lead = lead_ref[0]
    group, _, share = maps.shape[:3]
    later = (lead >> levels) & 1
    zero = jnp.zeros(far.shape[1:], BF16)
    es = [jnp.where(later == 0, far[i], zero) for i in range(share)]
    ss = [jnp.where(later == 0, zero, far[i]) for i in range(share)]
    for level in range(levels - 1, -1, -1):
        other = ranges[2 * level + 1]
        bit = (lead >> level) & 1
        for i in range(share):
            e = low(other[1, i].astype(F32) + dot(es[i], other[0, i]))
            s = low(other[2, i].astype(F32) + dot(other[0, i], ss[i]))
            es[i], ss[i] = jnp.where(bit == 0, e, es[i]), jnp.where(bit == 0, ss[i], s)
    for j in range(group):
        b = group - 1 - j
        for i in range(share):
            result[b, 0, i], result[j, 1, i] = es[i], ss[i]
            if j < group - 1:
                es[i] = low(maps[b, 1, i].astype(F32) + dot(es[i], maps[b, 0, i]))
                ss[i] = low(maps[j, 2, i].astype(F32) + dot(maps[j, 0, i], ss[i]))


def group_size(count, heads):
    size = 1
    while size * size < count and count % (2 * size) == 0 and heads % (2 * size) == 0:
        size *= 2
    return size


def per_device(queries, keys, hidden, value_weight, beta_pre, decay_pre, decay_rate, out_grad):
    heads = decay_rate.shape[0]
    n, width = queries.shape
    dk = width // heads
    dv = value_weight.shape[1] // heads
    model = hidden.shape[1]
    spans = lax.axis_size("sp")
    group = group_size(spans, heads)
    outer = spans // group
    place = lax.axis_index("sp")
    pos = lax.rem(place, group)
    lead = lax.div(place, group)
    lead_arr = jnp.full((1,), lead, jnp.int32)
    share = heads // group
    beta_t, decay_t = beta_pre.T, decay_pre.T
    big = heads * n * n * 256
    teams = [list(range(s, s + group)) for s in range(0, spans, group)]

    def swap(x):
        return lax.all_to_all(x, "sp", 0, 0, axis_index_groups=teams)

    def near(x, d):
        return lax.ppermute(x, "sp", [(s, s ^ d) for s in range(spans)]) if d else x

    def across(x, reach):
        return lax.ppermute(x, "sp", [(s, s ^ (reach * group)) for s in range(spans)])

    rows = model // spans
    col_scratch = [
        pltpu.VMEM((n, 128), F32), pltpu.VMEM((n, 128), F32), pltpu.VMEM((heads, n), F32)
    ]
    maps, inv, dr, y, bdr, by, values, *hidden_t = call(
        functools.partial(local_kernel, PACK, share, outer),
        [jnp.full((1,), pos, jnp.int32), queries, keys, out_grad, hidden, value_weight, beta_t, decay_t, decay_rate],
        [shape(group, 3, share, dk, dv), shape(heads, n, n)]
        + [shape(n, width)] * 5
        + [shape(outer * rows, n)] * group,
        col_scratch
        + [pltpu.VMEM(hidden.shape, BF16), pltpu.VMEM((model, n), BF16), pltpu.VMEM(value_weight.shape, BF16), pltpu.SemaphoreType.DMA((2,))],
        big,
        (4, 5),
    )
    small = group * share * dk * dk * dk * 4
    triple, single = shape(3, share, dk, dv), shape(share, dk, dv)

    maps = swap(maps)
    (total,) = call(total_kernel, [maps], [triple], (), small)
    levels = outer.bit_length() - 2
    ranges = []
    for level in range(levels):
        other = across(total, 1 << level)
        ranges += [total, other]
        last = level == levels - 1
        (total,) = call(
            functools.partial(join_kernel, level, last), [lead_arr, total, other],
            [single if last else triple], [pltpu.VMEM((2,) + triple.shape, BF16)], small,
        )
    far = across(total, 1 << levels)
    moved = []
    for d, part in enumerate(hidden_t):
        moved.append(near(part, d))
    hidden_t = moved
    (states,) = call(
        functools.partial(spread_kernel, levels), [lead_arr, maps, *ranges, far],
        [shape(group, 2, share, dk, dv)], (), small,
    )
    states = swap(states)

    chunk = width // CHUNKS
    d_values, *grad_chunks = call(
        functools.partial(values_kernel, share, CHUNKS),
        [bdr, by, states],
        [shape(n, width)] + [shape(n, chunk)] * CHUNKS,
        (),
        heads * n * dk * dv * 2,
    )
    pieces = []
    for own in grad_chunks:
        parts = []
        for d in range(group):
            parts.append(near(own, d))
        blocks = call(
            functools.partial(weight_kernel, group, outer),
            [lead_arr, *hidden_t, *parts],
            [shape(rows, chunk, dtype=BF16 if e else F32) for e in range(outer)],
            [pltpu.VMEM((outer * rows, chunk), F32)],
            2 * group * n * outer * rows * chunk,
        )
        for e, block in enumerate(blocks):
            step = [(s, (s + e * group) % spans) for s in range(spans)]
            pieces.append(lax.ppermute(block, "sp", step) if e else block)
    (d_weight,) = call(functools.partial(sum_kernel, outer), pieces, [shape(rows, width, dtype=F32)], (), rows * width)

    core = lax.axis_index("tp")
    cores = lax.axis_size("tp")
    own_rows = n // cores
    shares = call(
        functools.partial(input_kernel, cores),
        [jnp.full((1,), core, jnp.int32), d_values, value_weight],
        [shape(own_rows, model, dtype=BF16 if d else F32) for d in range(cores)],
        [pltpu.VMEM((n, model), F32)], n * width * model * 2,
    )
    shares = [
        lax.ppermute(x, "tp", [(c, (c + d) % cores) for c in range(cores)]) if d else x
        for d, x in enumerate(shares)
    ]
    (d_hidden,) = call(add_kernel, shares, [shape(own_rows, model)], (), own_rows * model)

    d_queries, d_keys, d_beta, d_decay = call(
        functools.partial(grads_kernel, PACK, share),
        [queries, keys, values, out_grad, beta_t, decay_t, decay_rate, inv, dr, y, states],
        [shape(n, width), shape(n, width), shape(heads, n, dtype=F32), shape(heads, n, dtype=F32)],
        col_scratch + [pltpu.VMEM((n, dk), F32), pltpu.VMEM((heads, n), F32), pltpu.VMEM((n, dk), F32)],
        big,
    )
    return (d_queries, d_keys, d_beta.T, d_decay.T, d_hidden, d_weight)


def solution(mesh):
    return jax.shard_map(
        per_device,
        mesh=mesh,
        in_specs=(
            P("sp", "tp"),
            P("sp", "tp"),
            P("sp", None),
            P(None, "tp"),
            P("sp", "tp"),
            P("sp", "tp"),
            P("tp"),
            P("sp", "tp"),
        ),
        out_specs=(
            P("sp", "tp"),
            P("sp", "tp"),
            P("sp", "tp"),
            P("sp", "tp"),
            P(("sp", "tp"), None),
            P("sp", "tp"),
        ),
        check_vma=False,
    )
```

```python
import functools

import jax
import jax.numpy as jnp
from jax import lax
from jax.experimental import pallas as pl
from jax.experimental.pallas import tpu as pltpu
from jax.sharding import PartitionSpec as P


NORM_FLOOR = 16.0
F32 = jnp.float32
BF16 = jnp.bfloat16
HIGHEST = lax.Precision.HIGHEST
MIB = 1024 * 1024
VMEM = {"local": 56, "grads": 28, "weight": 8, "input": 14}
PACK = 8
CHUNKS = 2


def dot(a, b, ca=1, cb=0, precision=None):
    return lax.dot_general(
        a, b, (((ca,), (cb,)), ((), ())), precision=precision, preferred_element_type=F32
    )


def low(x):
    return x.astype(BF16)


def iotas(n):
    rows = lax.broadcasted_iota(jnp.int32, (n, n), 0)
    cols = lax.broadcasted_iota(jnp.int32, (n, n), 1)
    return rows, cols


def columns(rows):
    count, n = rows.shape
    return jnp.transpose(jnp.concatenate([rows, jnp.zeros((128 - count, n), F32)], axis=0))


def rate_column(rate_ref):
    count = rate_ref.shape[0]
    row = lax.broadcasted_iota(jnp.int32, (count, 1), 0)
    out = jnp.zeros((count, 1), F32)
    for h in range(count):
        out = jnp.where(row == h, rate_ref[h], out)
    return out


def sigmoid(x):
    return 1.0 / (1.0 + jnp.exp(-x))


def head_columns(beta_ref, decay_ref, rate_ref, g_ref, b_ref, gt_ref):
    decay = decay_ref[...]
    n = decay.shape[1]
    rows, cols = iotas(n)
    log_decay = -rate_column(rate_ref) * (
        jnp.maximum(decay, 0.0) + jnp.log1p(jnp.exp(-jnp.abs(decay)))
    )
    sums = dot(log_decay, (rows <= cols).astype(F32), precision=HIGHEST)
    gt_ref[...] = sums
    g_ref[...] = columns(sums)
    b_ref[...] = columns(sigmoid(beta_ref[...]))


def lane_column(ref, head):
    return jnp.broadcast_to(ref[:, head : head + 1], ref.shape)


class Head:
    pass


def lanes_of(head, size):
    return slice(head * size, (head + 1) * size)


def head_common(q_ref, k_ref, head, size, g_ref, b_ref, gt_ref):
    h = Head()
    n = q_ref.shape[0]
    h.head, h.n, h.size = head, n, size
    h.lanes = lanes_of(head, size)
    h.k16, h.q16 = k_ref[:, h.lanes], q_ref[:, h.lanes]
    k32, q32 = h.k16.astype(F32), h.q16.astype(F32)
    h.g = lane_column(g_ref, head)
    h.beta = lane_column(b_ref, head)
    norm = lambda x: jnp.broadcast_to(
        lax.rsqrt(jnp.sum(x * x, axis=1, keepdims=True) + NORM_FLOOR), (n, size)
    )
    h.rk, h.rq = norm(k32), norm(q32)
    g_row = gt_ref[head : head + 1, :]
    rk_row = jnp.transpose(h.rk)[0:1, :]
    rows, cols = iotas(n)
    h.tile = lambda x: jnp.concatenate([x] * (n // size), axis=1)
    spread = jnp.where(rows >= cols, h.tile(h.g) - g_row, -1e30)
    h.gamma_rk = jnp.exp(spread) * rk_row
    gram = dot(jnp.concatenate([h.k16, h.q16], axis=0), h.k16, 1, 1)
    h.scale = size**-0.5
    h.a0 = jnp.where(rows > cols, gram[:n] * h.gamma_rk * h.tile(h.rk), 0.0)
    h.p = gram[n:] * h.gamma_rk * h.tile(h.rq * h.scale)
    g_end = h.g[n - 1 : n, :]
    h.k_hat, h.q_hat = k32 * h.rk, q32 * (h.rq * h.scale)
    h.gain, h.tail, h.gain_end = jnp.exp(h.g), jnp.exp(g_end - h.g), jnp.exp(g_end)
    return h


def unit_lower_inverses(mats):
    n = mats[0].shape[0]
    rows, cols = iotas(n)
    differ = rows ^ cols
    eye = (rows == cols).astype(F32)
    high = [low(a) for a in mats]
    xs = [low(eye) - a * low((differ == 1).astype(F32)) for a in high]
    size = 2
    while 2 * size < n:
        mask = low(((differ >= size) & (differ < 2 * size)).astype(F32))
        ys = [low(dot(a * mask, x)) for a, x in zip(high, xs)]
        xs = [x - low(dot(x, y)) for x, y in zip(xs, ys)]
        size *= 2
    ys = [low(dot(a[size:, :size], x[:size, :size])) for a, x in zip(high, xs)]
    zs = [low(-dot(x[size:, size:], y)) for x, y in zip(xs, ys)]
    xs = [
        jnp.concatenate([x[:size], jnp.concatenate([z, x[size:, size:]], axis=1)], axis=0)
        for x, z in zip(xs, zs)
    ]
    rest = [low(a - h.astype(F32)) for a, h in zip(mats, high)]
    products = [
        dot(jnp.concatenate([h, l], axis=1), jnp.concatenate([x, x], axis=0))
        for h, l, x in zip(high, rest, xs)
    ]
    return [
        low(x.astype(F32) + dot(x, low(eye - x.astype(F32) - y))) for x, y in zip(xs, products)
    ]


def local_kernel(pack, share, outer, pos_ref, q_hbm, k_hbm, do_hbm, hid_ref, w_ref, bp_ref, dp_ref, rate_ref, maps,
                 *refs):
    inv_ref, dr_ref, y_ref, bdr_ref, by_ref, v_ref, g_ref, b_ref, gt_ref, q_ref, k_ref, do_ref, hid, hid_t, w, sems = refs[: 6] + refs[6 + maps.shape[0] :]
    hid_parts = refs[6 : 6 + maps.shape[0]]
    pairs = [(k_hbm, k_ref), (q_hbm, q_ref), (do_hbm, do_ref), (hid_ref, hid), (w_ref, w)]
    copies = [pltpu.make_async_copy(a, b, sems.at[i]) for i, (a, b) in enumerate(pairs)]
    for copy in copies:
        copy.start()
    head_columns(bp_ref, dp_ref, rate_ref, g_ref, b_ref, gt_ref)
    for copy in copies[:3]:
        copy.wait()
    size = maps.shape[-1]
    for start in range(0, maps.shape[0] * share, pack):
        places = range(start, start + pack)
        heads = [head_common(q_ref, k_ref, p, size, g_ref, b_ref, gt_ref) for p in places]
        outs = [do_ref[:, h.lanes] for h in heads]
        d_written = [low(dot(low(h.p), do16, 0, 0)) for h, do16 in zip(heads, outs)]
        invs = unit_lower_inverses([h.a0 * h.tile(h.beta) for h in heads])
        tails = [low(h.k_hat * h.tail) for h in heads]
        both = [
            dot(inv, jnp.concatenate([d, t], axis=1), 0, 0)
            for inv, d, t in zip(invs, d_written, tails)
        ]
        if start == 0:
            for copy in copies[3:]:
                copy.wait()
            v_ref[...] = low(dot(hid[...], w[...]))
            rows = hid.shape[1] // outer // maps.shape[0]
            hid_t[...] = jnp.transpose(hid[...])
            for d, part in enumerate(hid_parts):
                for e in range(outer):
                    at = pl.multiple_of((e * maps.shape[0] + (pos_ref[0] ^ d)) * rows, rows)
                    part[e * rows : (e + 1) * rows, :] = hid_t[pl.ds(at, rows), :]
        eye = lax.broadcasted_iota(jnp.int32, (size, size), 0) == lax.broadcasted_iota(
            jnp.int32, (size, size), 1
        )
        for p, h, inv, do16, b32 in zip(places, heads, invs, outs, both):
            dr16, y16 = low(b32[:, :size]), low(b32[:, size:])
            inv_ref[p] = inv
            dr_ref[:, h.lanes] = dr16
            y_ref[:, h.lanes] = y16
            bdr_ref[:, h.lanes] = low(h.beta * b32[:, :size])
            by_ref[:, h.lanes] = low(h.beta * b32[:, size:])
            k_in = low(h.k_hat * h.beta * h.gain)
            value = low(h.beta * v_ref[:, h.lanes].astype(F32))
            out = maps.at[p // share]
            into = dot(y16, jnp.concatenate([k_in, value], axis=1), 0, 0)
            out[0, p % share] = low(jnp.where(eye, h.gain_end, 0.0) - into[:, :size])
            own = dot(
                jnp.concatenate([do16, dr16], axis=0),
                jnp.concatenate([low(h.q_hat * h.gain), -k_in], axis=0), 0, 0,
            )
            out[1, p % share] = low(own)
            out[2, p % share] = low(into[:, size:])


def values_kernel(share, chunks, bdr_ref, by_ref, states, dv_ref, *parts):
    size = states.shape[-1]
    count = states.shape[0] * share
    per = count // chunks
    for h in range(count):
        lanes = slice(h * size, (h + 1) * size)
        dv = low(bdr_ref[:, lanes].astype(F32) + dot(by_ref[:, lanes], states[h // share, 0, h % share], 1, 1))
        dv_ref[:, lanes] = dv
        parts[h // per][:, (h % per) * size : (h % per + 1) * size] = dv


def weight_kernel(group, outer, lead_ref, *refs):
    hid_refs, grad_refs, out_refs, store = refs[:group], refs[group : 2 * group], refs[2 * group : -1], refs[-1]
    rows = store.shape[0] // outer
    store[...] = dot(
        jnp.concatenate([r[...] for r in hid_refs], axis=1),
        jnp.concatenate([r[...] for r in grad_refs], axis=0),
    )
    lead = lead_ref[0]
    for e in range(outer):
        block = store[pl.ds(pl.multiple_of((lead ^ e) * rows, rows), rows), :]
        out_refs[e][...] = block.astype(out_refs[e].dtype)


def input_kernel(cores, core_ref, dv_ref, w_ref, *refs):
    out_refs, store = refs[:-1], refs[-1]
    rows = dv_ref.shape[0] // cores
    core = core_ref[0]
    store[...] = dot(dv_ref[...], w_ref[...], 1, 1)
    for d, out_ref in enumerate(out_refs):
        start = pl.multiple_of(lax.rem(core + d, cores) * rows, rows)
        out_ref[...] = store[pl.ds(start, rows), :].astype(out_ref.dtype)


def add_kernel(*refs):
    refs[-1][...] = low(sum(r[...].astype(F32) for r in refs[:-1]))


def sum_kernel(outer, *refs):
    out_ref = refs[-1]
    chunks = (len(refs) - 1) // outer
    width = refs[0].shape[1]
    for c in range(chunks):
        parts = refs[c * outer : (c + 1) * outer]
        out_ref[:, c * width : (c + 1) * width] = sum(r[...].astype(F32) for r in parts)


def grads_kernel(pack, share, q_ref, k_ref, v_ref, do_ref, bp_ref, dp_ref, rate_ref, inv_ref, dr_ref, y_ref, states,
                 dq_ref, dk_ref, db_ref, dd_ref, g_ref, b_ref, gt_ref, row_acc, col_acc, db_acc):
    size = states.shape[-1]
    head_columns(bp_ref, dp_ref, rate_ref, g_ref, b_ref, gt_ref)
    count = states.shape[0] * share
    n = q_ref.shape[0]
    rows, cols = iotas(n)
    lane = lax.broadcasted_iota(jnp.int32, (n, size), 1)
    row_acc[...] = jnp.zeros_like(row_acc)
    db_acc[...] = jnp.zeros_like(db_acc)
    for start in range(0, count, pack):
        places = range(start, start + pack)
        heads = [head_common(q_ref, k_ref, p, size, g_ref, b_ref, gt_ref) for p in places]
        for p, h in zip(places, heads):
            h.e16, h.s16 = states[p // share, 0, p % share], states[p // share, 1, p % share]
            h.do16 = do_ref[:, h.lanes]
            inner = v_ref[:, h.lanes].astype(F32) - h.gain * (h.rk * dot(h.k16, h.s16))
            h.right = low(h.beta * inner)
            h.dr = dr_ref[:, h.lanes].astype(F32) + dot(y_ref[:, h.lanes], h.e16, 1, 1)
            h.dr16 = low(h.dr)
        for p, h in zip(places, heads):
            h.written = dot(inv_ref[p], h.right)
            h.w16 = low(h.written)
            at_s = dot(jnp.concatenate([h.do16, h.dr16], axis=0), h.s16, 1, 1)
            h.d_qd, h.dr_s = at_s[:n], at_s[n:]
        for h in heads:
            pair = dot(jnp.concatenate([-h.dr16, h.do16], axis=0), h.w16, 1, 1)
            d_a, d_p = pair[:n], pair[n:]
            h.weights = d_a * h.a0 * h.tile(h.beta) + d_p * h.p
            x1 = low(jnp.where(rows > cols, d_a * h.gamma_rk, 0.0))
            x2 = low(d_p * h.gamma_rk)
            h.xs = jnp.concatenate([x1, x2], axis=0)
            h.d_kt = dot(h.w16, h.e16)
        for h in heads:
            row_side = dot(h.xs, h.k16)
            col_side = dot(
                h.xs, jnp.concatenate([low(h.beta * h.k_hat), low(h.q_hat)], axis=0), 0, 0
            )
            d_q = row_side[n:] + h.gain * h.d_qd
            in_term = h.beta * h.gain * h.dr_s
            d_k = h.rk * (h.beta * row_side[:n] - in_term + h.tail * h.d_kt) + col_side
            unit = h.q16.astype(F32) * h.rq
            d_q = h.rq * h.scale * (d_q - unit * jnp.sum(unit * d_q, axis=1, keepdims=True))
            d_k = d_k - h.k_hat * jnp.sum(h.k_hat * d_k, axis=1, keepdims=True)
            dq_ref[:, h.lanes] = low(d_q)
            dk_ref[:, h.lanes] = low(d_k)
            tail_term = h.d_kt * h.k_hat * h.tail
            direct = h.gain * h.d_qd * h.q_hat - in_term * h.k_hat - tail_term
            folded = sum(h.weights[:, i * size : (i + 1) * size] for i in range(n // size))
            row_sum = jnp.sum(folded + direct, axis=1, keepdims=True)
            end = jnp.sum(
                jnp.sum(tail_term, axis=0, keepdims=True)
                + jnp.sum(h.gain_end * (h.s16.astype(F32) * jnp.transpose(h.e16.astype(F32))), axis=0, keepdims=True),
                axis=1, keepdims=True,
            )
            last = lax.broadcasted_iota(jnp.int32, (1, n), 1) == n - 1
            col_acc[h.head : h.head + 1, :] = jnp.where(last, end, 0.0) - jnp.sum(
                h.weights, axis=0, keepdims=True
            )
            row_acc[...] = jnp.where(lane == h.head, row_sum, row_acc[...])
            d_beta = (1.0 - h.beta) * jnp.sum(h.dr * h.written, axis=1, keepdims=True)
            db_acc[...] = jnp.where(lane == h.head, d_beta, db_acc[...])
    d_sums = jnp.transpose(row_acc[...])[0:count] + col_acc[...]
    d_log = dot(d_sums, (rows >= cols).astype(F32), precision=HIGHEST)
    dd_ref[...] = -rate_column(rate_ref) * sigmoid(dp_ref[...]) * d_log
    db_ref[...] = jnp.transpose(db_acc[...])[0:count]


def call(body, name, args, outs, scratch=(), flops=0, anywhere=()):
    def place(i, a):
        space = pltpu.SMEM if a.ndim == 1 else pltpu.HBM if i in anywhere else pltpu.VMEM
        return pl.BlockSpec(memory_space=space)

    return pl.pallas_call(
        body,
        in_specs=[place(i, a) for i, a in enumerate(args)],
        out_specs=[pl.BlockSpec(memory_space=pltpu.VMEM) for _ in outs],
        out_shape=outs,
        scratch_shapes=list(scratch),
        compiler_params=pltpu.CompilerParams(vmem_limit_bytes=VMEM.get(name, 6) * MIB),
        cost_estimate=pl.CostEstimate(flops=flops, bytes_accessed=1 << 20, transcendentals=0),
    )(*args)


def shape(*dims, dtype=BF16):
    return jax.ShapeDtypeStruct(dims, dtype)


def total_kernel(maps, total_ref):
    group, _, share = maps.shape[:3]
    for i in range(share):
        g, o, t = maps[group - 1, 1, i], maps[0, 2, i], maps[0, 0, i]
        for j in range(1, group):
            b = group - 1 - j
            g = low(maps[b, 1, i].astype(F32) + dot(g, maps[b, 0, i]))
            o = low(maps[j, 2, i].astype(F32) + dot(maps[j, 0, i], o))
            t = low(dot(maps[j, 0, i], t))
        total_ref[0, i], total_ref[1, i], total_ref[2, i] = t, g, o


def join_kernel(level, last, lead_ref, own, other, out_ref, both):
    lead = lead_ref[0]
    bit = (lead >> level) & 1
    both[bit] = own[...]
    both[1 - bit] = other[...]
    for i in range(own.shape[1]):
        g = low(both[0, 1, i].astype(F32) + dot(both[1, 1, i], both[0, 0, i]))
        o = low(both[1, 2, i].astype(F32) + dot(both[1, 0, i], both[0, 2, i]))
        if last:
            out_ref[i] = jnp.where((lead >> (level + 1)) & 1 == 0, o, g)
        else:
            out_ref[0, i], out_ref[1, i], out_ref[2, i] = low(dot(both[1, 0, i], both[0, 0, i])), g, o


def spread_kernel(levels, lead_ref, maps, *refs):
    ranges, far, result = refs[: 2 * levels], refs[2 * levels], refs[2 * levels + 1]
    lead = lead_ref[0]
    group, _, share = maps.shape[:3]
    later = (lead >> levels) & 1
    zero = jnp.zeros(far.shape[1:], BF16)
    es = [jnp.where(later == 0, far[i], zero) for i in range(share)]
    ss = [jnp.where(later == 0, zero, far[i]) for i in range(share)]
    for level in range(levels - 1, -1, -1):
        other = ranges[2 * level + 1]
        bit = (lead >> level) & 1
        for i in range(share):
            e = low(other[1, i].astype(F32) + dot(es[i], other[0, i]))
            s = low(other[2, i].astype(F32) + dot(other[0, i], ss[i]))
            es[i], ss[i] = jnp.where(bit == 0, e, es[i]), jnp.where(bit == 0, ss[i], s)
    for j in range(group):
        b = group - 1 - j
        for i in range(share):
            result[b, 0, i], result[j, 1, i] = es[i], ss[i]
            if j < group - 1:
                es[i] = low(maps[b, 1, i].astype(F32) + dot(es[i], maps[b, 0, i]))
                ss[i] = low(maps[j, 2, i].astype(F32) + dot(maps[j, 0, i], ss[i]))


def group_size(count, heads):
    size = 1
    while size * size < count and count % (2 * size) == 0 and heads % (2 * size) == 0:
        size *= 2
    return size


def per_device(queries, keys, hidden, value_weight, beta_pre, decay_pre, decay_rate, out_grad):
    heads = decay_rate.shape[0]
    n, width = queries.shape
    dk = width // heads
    dv = value_weight.shape[1] // heads
    model = hidden.shape[1]
    spans = lax.axis_size("sp")
    group = group_size(spans, heads)
    outer = spans // group
    place = lax.axis_index("sp")
    pos = lax.rem(place, group)
    lead = lax.div(place, group)
    lead_arr = jnp.full((1,), lead, jnp.int32)
    share = heads // group
    beta_t, decay_t = beta_pre.T, decay_pre.T
    big = heads * n * n * 256
    teams = [list(range(s, s + group)) for s in range(0, spans, group)]

    def swap(x):
        return lax.all_to_all(x, "sp", 0, 0, axis_index_groups=teams)

    def near(x, d):
        return lax.ppermute(x, "sp", [(s, s ^ d) for s in range(spans)]) if d else x

    def across(x, reach):
        return lax.ppermute(x, "sp", [(s, s ^ (reach * group)) for s in range(spans)])

    rows = model // spans
    col_scratch = [
        pltpu.VMEM((n, 128), F32), pltpu.VMEM((n, 128), F32), pltpu.VMEM((heads, n), F32)
    ]
    maps, inv, dr, y, bdr, by, values, *hidden_t = call(
        functools.partial(local_kernel, PACK, share, outer),
        "local",
        [jnp.full((1,), pos, jnp.int32), queries, keys, out_grad, hidden, value_weight, beta_t, decay_t, decay_rate],
        [shape(group, 3, share, dk, dv), shape(heads, n, n)]
        + [shape(n, width)] * 5
        + [shape(outer * rows, n)] * group,
        col_scratch
        + [pltpu.VMEM((n, width), BF16)] * 3
        + [pltpu.VMEM(hidden.shape, BF16), pltpu.VMEM((model, n), BF16), pltpu.VMEM(value_weight.shape, BF16), pltpu.SemaphoreType.DMA((5,))],
        big,
        (1, 2, 3, 4, 5),
    )
    small = group * share * dk * dk * dk * 4
    triple, single = shape(3, share, dk, dv), shape(share, dk, dv)

    maps = swap(maps)
    (total,) = call(total_kernel, "total", [maps], [triple], (), small)
    levels = outer.bit_length() - 2
    ranges = []
    for level in range(levels):
        other = across(total, 1 << level)
        ranges += [total, other]
        last = level == levels - 1
        (total,) = call(
            functools.partial(join_kernel, level, last), "join", [lead_arr, total, other],
            [single if last else triple], [pltpu.VMEM((2,) + triple.shape, BF16)], small,
        )
    far = across(total, 1 << levels)
    moved = []
    for d, part in enumerate(hidden_t):
        moved.append(near(part, d))
    hidden_t = moved
    (states,) = call(
        functools.partial(spread_kernel, levels), "spread", [lead_arr, maps, *ranges, far],
        [shape(group, 2, share, dk, dv)], (), small,
    )
    states = swap(states)

    chunk = width // CHUNKS
    d_values, *grad_chunks = call(
        functools.partial(values_kernel, share, CHUNKS),
        "values",
        [bdr, by, states],
        [shape(n, width)] + [shape(n, chunk)] * CHUNKS,
        (),
        heads * n * dk * dv * 2,
    )
    pieces = []
    for own in grad_chunks:
        parts = []
        for d in range(group):
            parts.append(near(own, d))
        blocks = call(
            functools.partial(weight_kernel, group, outer),
            "weight",
            [lead_arr, *hidden_t, *parts],
            [shape(rows, chunk, dtype=BF16 if e else F32) for e in range(outer)],
            [pltpu.VMEM((outer * rows, chunk), F32)],
            2 * group * n * outer * rows * chunk,
        )
        for e, block in enumerate(blocks):
            pieces.append(across(block, e) if e else block)
    (d_weight,) = call(
        functools.partial(sum_kernel, outer), "sum", pieces, [shape(rows, width, dtype=F32)], (), rows * width
    )

    core = lax.axis_index("tp")
    cores = lax.axis_size("tp")
    own_rows = n // cores
    shares = call(
        functools.partial(input_kernel, cores), "input",
        [jnp.full((1,), core, jnp.int32), d_values, value_weight],
        [shape(own_rows, model, dtype=BF16 if d else F32) for d in range(cores)],
        [pltpu.VMEM((n, model), F32)], n * width * model * 2,
    )
    shares = [
        lax.ppermute(x, "tp", [(c, (c + d) % cores) for c in range(cores)]) if d else x
        for d, x in enumerate(shares)
    ]
    (d_hidden,) = call(add_kernel, "add", shares, [shape(own_rows, model)], (), own_rows * model)

    d_queries, d_keys, d_beta, d_decay = call(
        functools.partial(grads_kernel, PACK, share),
        "grads",
        [queries, keys, values, out_grad, beta_t, decay_t, decay_rate, inv, dr, y, states],
        [shape(n, width), shape(n, width), shape(heads, n, dtype=F32), shape(heads, n, dtype=F32)],
        col_scratch + [pltpu.VMEM((n, dk), F32), pltpu.VMEM((heads, n), F32), pltpu.VMEM((n, dk), F32)],
        big,
    )
    return (d_queries, d_keys, d_beta.T, d_decay.T, d_hidden, d_weight)


def solution(mesh):
    return jax.shard_map(
        per_device,
        mesh=mesh,
        in_specs=(
            P("sp", "tp"),
            P("sp", "tp"),
            P("sp", None),
            P(None, "tp"),
            P("sp", "tp"),
            P("sp", "tp"),
            P("tp"),
            P("sp", "tp"),
        ),
        out_specs=(
            P("sp", "tp"),
            P("sp", "tp"),
            P("sp", "tp"),
            P("sp", "tp"),
            P(("sp", "tp"), None),
            P("sp", "tp"),
        ),
        check_vma=False,
    )
```

```python
import functools

import jax
import jax.numpy as jnp
from jax import lax
from jax.experimental import pallas as pl
from jax.experimental.pallas import tpu as pltpu
from jax.sharding import PartitionSpec as P


NORM_FLOOR = 16.0
F32 = jnp.float32
BF16 = jnp.bfloat16
HIGHEST = lax.Precision.HIGHEST
MIB = 1024 * 1024
VMEM = {"local": 56, "grads": 28, "weight": 8, "input": 14}
PACK = 8


def dot(a, b, ca=1, cb=0, precision=None):
    return lax.dot_general(
        a, b, (((ca,), (cb,)), ((), ())), precision=precision, preferred_element_type=F32
    )


def low(x):
    return x.astype(BF16)


def iotas(n):
    rows = lax.broadcasted_iota(jnp.int32, (n, n), 0)
    cols = lax.broadcasted_iota(jnp.int32, (n, n), 1)
    return rows, cols


def columns(rows):
    count, n = rows.shape
    return jnp.transpose(jnp.concatenate([rows, jnp.zeros((128 - count, n), F32)], axis=0))


def rate_column(rate_ref):
    count = rate_ref.shape[0]
    row = lax.broadcasted_iota(jnp.int32, (count, 1), 0)
    out = jnp.zeros((count, 1), F32)
    for h in range(count):
        out = jnp.where(row == h, rate_ref[h], out)
    return out


def sigmoid(x):
    return 1.0 / (1.0 + jnp.exp(-x))


def head_columns(beta_ref, decay_ref, rate_ref, g_ref, b_ref, gt_ref):
    decay = decay_ref[...]
    n = decay.shape[1]
    rows, cols = iotas(n)
    log_decay = -rate_column(rate_ref) * (
        jnp.maximum(decay, 0.0) + jnp.log1p(jnp.exp(-jnp.abs(decay)))
    )
    sums = dot(log_decay, (rows <= cols).astype(F32), precision=HIGHEST)
    gt_ref[...] = sums
    g_ref[...] = columns(sums)
    b_ref[...] = columns(sigmoid(beta_ref[...]))


def lane_column(ref, head):
    return jnp.broadcast_to(ref[:, head : head + 1], ref.shape)


class Head:
    pass


def lanes_of(head, size):
    return slice(head * size, (head + 1) * size)


def head_common(q_ref, k_ref, head, size, g_ref, b_ref, gt_ref):
    h = Head()
    n = q_ref.shape[0]
    h.head, h.n, h.size = head, n, size
    h.lanes = lanes_of(head, size)
    h.k16, h.q16 = k_ref[:, h.lanes], q_ref[:, h.lanes]
    k32, q32 = h.k16.astype(F32), h.q16.astype(F32)
    h.g = lane_column(g_ref, head)
    h.beta = lane_column(b_ref, head)
    norm = lambda x: jnp.broadcast_to(
        lax.rsqrt(jnp.sum(x * x, axis=1, keepdims=True) + NORM_FLOOR), (n, size)
    )
    h.rk, h.rq = norm(k32), norm(q32)
    g_row = gt_ref[head : head + 1, :]
    rk_row = jnp.transpose(h.rk)[0:1, :]
    rows, cols = iotas(n)
    h.tile = lambda x: jnp.concatenate([x] * (n // size), axis=1)
    spread = jnp.where(rows >= cols, h.tile(h.g) - g_row, -1e30)
    h.gamma_rk = jnp.exp(spread) * rk_row
    gram = dot(jnp.concatenate([h.k16, h.q16], axis=0), h.k16, 1, 1)
    h.scale = size**-0.5
    h.a0 = jnp.where(rows > cols, gram[:n] * h.gamma_rk * h.tile(h.rk), 0.0)
    h.p = gram[n:] * h.gamma_rk * h.tile(h.rq * h.scale)
    g_end = h.g[n - 1 : n, :]
    h.k_hat, h.q_hat = k32 * h.rk, q32 * (h.rq * h.scale)
    h.gain, h.tail, h.gain_end = jnp.exp(h.g), jnp.exp(g_end - h.g), jnp.exp(g_end)
    return h


def unit_lower_inverses(high):
    n = high[0].shape[0]
    rows, cols = iotas(n)
    differ = rows ^ cols
    eye = (rows == cols).astype(F32)
    xs = [low(eye) - a * low((differ == 1).astype(F32)) for a in high]
    size = 2
    while 2 * size < n:
        mask = low(((differ >= size) & (differ < 2 * size)).astype(F32))
        ys = [low(dot(a * mask, x)) for a, x in zip(high, xs)]
        xs = [x - low(dot(x, y)) for x, y in zip(xs, ys)]
        size *= 2
    ys = [low(dot(a[size:, :size], x[:size, :size])) for a, x in zip(high, xs)]
    zs = [low(-dot(x[size:, size:], y)) for x, y in zip(xs, ys)]
    xs = [
        jnp.concatenate([x[:size], jnp.concatenate([z, x[size:, size:]], axis=1)], axis=0)
        for x, z in zip(xs, zs)
    ]
    rests = [low(eye - x.astype(F32) - dot(a, x)) for a, x in zip(high, xs)]
    return [low(x.astype(F32) + dot(x, r)) for x, r in zip(xs, rests)]


def local_kernel(pack, share, outer, pos_ref, q_hbm, k_hbm, do_hbm, hid_ref, w_ref, bp_ref, dp_ref, rate_ref, maps,
                 *refs):
    inv_ref, dr_ref, y_ref, bdr_ref, by_ref, v_ref, g_ref, b_ref, gt_ref, q_ref, k_ref, do_ref, hid, hid_t, w, sems = refs[: 6] + refs[6 + maps.shape[0] :]
    hid_parts = refs[6 : 6 + maps.shape[0]]
    pairs = [(k_hbm, k_ref), (q_hbm, q_ref), (do_hbm, do_ref), (hid_ref, hid), (w_ref, w)]
    copies = [pltpu.make_async_copy(a, b, sems.at[i]) for i, (a, b) in enumerate(pairs)]
    for copy in copies:
        copy.start()
    head_columns(bp_ref, dp_ref, rate_ref, g_ref, b_ref, gt_ref)
    for copy in copies[:3]:
        copy.wait()
    size = maps.shape[-1]
    for start in range(0, maps.shape[0] * share, pack):
        places = range(start, start + pack)
        heads = [head_common(q_ref, k_ref, p, size, g_ref, b_ref, gt_ref) for p in places]
        outs = [do_ref[:, h.lanes] for h in heads]
        d_written = [low(dot(low(h.p), do16, 0, 0)) for h, do16 in zip(heads, outs)]
        invs = unit_lower_inverses([low(h.a0 * h.tile(h.beta)) for h in heads])
        tails = [low(h.k_hat * h.tail) for h in heads]
        both = [
            dot(inv, jnp.concatenate([d, t], axis=1), 0, 0)
            for inv, d, t in zip(invs, d_written, tails)
        ]
        if start == 0:
            for copy in copies[3:]:
                copy.wait()
            v_ref[...] = low(dot(hid[...], w[...]))
            rows = hid.shape[1] // outer // maps.shape[0]
            hid_t[...] = jnp.transpose(hid[...])
            for d, part in enumerate(hid_parts):
                for e in range(outer):
                    at = pl.multiple_of((e * maps.shape[0] + (pos_ref[0] ^ d)) * rows, rows)
                    part[e * rows : (e + 1) * rows, :] = hid_t[pl.ds(at, rows), :]
        eye = lax.broadcasted_iota(jnp.int32, (size, size), 0) == lax.broadcasted_iota(
            jnp.int32, (size, size), 1
        )
        for p, h, inv, do16, b32 in zip(places, heads, invs, outs, both):
            dr16, y16 = low(b32[:, :size]), low(b32[:, size:])
            inv_ref[p] = inv
            dr_ref[:, h.lanes] = dr16
            y_ref[:, h.lanes] = y16
            bdr_ref[:, h.lanes] = low(h.beta * b32[:, :size])
            by_ref[:, h.lanes] = low(h.beta * b32[:, size:])
            k_in = low(h.k_hat * h.beta * h.gain)
            value = low(h.beta * v_ref[:, h.lanes].astype(F32))
            out = maps.at[p // share]
            into = dot(y16, jnp.concatenate([k_in, value], axis=1), 0, 0)
            out[0, p % share] = low(jnp.where(eye, h.gain_end, 0.0) - into[:, :size])
            own = dot(
                jnp.concatenate([do16, dr16], axis=0),
                jnp.concatenate([low(h.q_hat * h.gain), -k_in], axis=0), 0, 0,
            )
            out[1, p % share] = low(own)
            out[2, p % share] = low(into[:, size:])


def values_kernel(share, group, pos_ref, bdr_ref, by_ref, *refs):
    state_refs, states, dv_ref, parts = refs[:group], refs[group], refs[group + 1], refs[group + 2 :]
    for d, ref in enumerate(state_refs):
        states[pos_ref[0] ^ d] = ref[...]
    size = states.shape[-1]
    count = states.shape[0] * share
    places = [(part, i) for part in parts for i in range(part.shape[1] // size)]
    for h in range(count):
        lanes = slice(h * size, (h + 1) * size)
        dv = low(bdr_ref[:, lanes].astype(F32) + dot(by_ref[:, lanes], states[h // share, 0, h % share], 1, 1))
        dv_ref[:, lanes] = dv
        part, i = places[h]
        part[:, i * size : (i + 1) * size] = dv


def weight_kernel(group, outer, lead_ref, *refs):
    hid_refs, grad_refs, out_refs, store = refs[:group], refs[group : 2 * group], refs[2 * group : -1], refs[-1]
    rows = store.shape[0] // outer
    store[...] = dot(
        jnp.concatenate([r[...] for r in hid_refs], axis=1),
        jnp.concatenate([r[...] for r in grad_refs], axis=0),
    )
    lead = lead_ref[0]
    for e in range(outer):
        block = store[pl.ds(pl.multiple_of((lead ^ e) * rows, rows), rows), :]
        out_refs[e][...] = block.astype(out_refs[e].dtype)


def input_kernel(cores, core_ref, dv_ref, w_ref, *refs):
    out_refs, store = refs[:-1], refs[-1]
    rows = dv_ref.shape[0] // cores
    core = core_ref[0]
    store[...] = dot(dv_ref[...], w_ref[...], 1, 1)
    for d, out_ref in enumerate(out_refs):
        start = pl.multiple_of(lax.rem(core + d, cores) * rows, rows)
        out_ref[...] = store[pl.ds(start, rows), :].astype(out_ref.dtype)


def add_kernel(*refs):
    refs[-1][...] = low(sum(r[...].astype(F32) for r in refs[:-1]))


def sum_kernel(outer, *refs):
    out_ref = refs[-1]
    at = 0
    for c in range(0, len(refs) - 1, outer):
        parts = refs[c : c + outer]
        width = parts[0].shape[1]
        out_ref[:, at : at + width] = sum(r[...].astype(F32) for r in parts)
        at += width


def grads_kernel(pack, share, q_ref, k_ref, v_ref, do_ref, bp_ref, dp_ref, rate_ref, inv_ref, dr_ref, y_ref, states,
                 dq_ref, dk_ref, db_ref, dd_ref, g_ref, b_ref, gt_ref, row_acc, col_acc, db_acc):
    size = states.shape[-1]
    head_columns(bp_ref, dp_ref, rate_ref, g_ref, b_ref, gt_ref)
    count = states.shape[0] * share
    n = q_ref.shape[0]
    rows, cols = iotas(n)
    lane = lax.broadcasted_iota(jnp.int32, (n, size), 1)
    row_acc[...] = jnp.zeros_like(row_acc)
    db_acc[...] = jnp.zeros_like(db_acc)
    for start in range(0, count, pack):
        places = range(start, start + pack)
        heads = [head_common(q_ref, k_ref, p, size, g_ref, b_ref, gt_ref) for p in places]
        for p, h in zip(places, heads):
            h.e16, h.s16 = states[p // share, 0, p % share], states[p // share, 1, p % share]
            h.do16 = do_ref[:, h.lanes]
            inner = v_ref[:, h.lanes].astype(F32) - h.gain * (h.rk * dot(h.k16, h.s16))
            h.right = low(h.beta * inner)
            h.dr = dr_ref[:, h.lanes].astype(F32) + dot(y_ref[:, h.lanes], h.e16, 1, 1)
            h.dr16 = low(h.dr)
        for p, h in zip(places, heads):
            h.written = dot(inv_ref[p], h.right)
            h.w16 = low(h.written)
            at_s = dot(jnp.concatenate([h.do16, h.dr16], axis=0), h.s16, 1, 1)
            h.d_qd, h.dr_s = at_s[:n], at_s[n:]
        for h in heads:
            pair = dot(jnp.concatenate([-h.dr16, h.do16], axis=0), h.w16, 1, 1)
            d_a, d_p = pair[:n], pair[n:]
            h.weights = d_a * h.a0 * h.tile(h.beta) + d_p * h.p
            x1 = low(jnp.where(rows > cols, d_a * h.gamma_rk, 0.0))
            x2 = low(d_p * h.gamma_rk)
            h.xs = jnp.concatenate([x1, x2], axis=0)
            h.d_kt = dot(h.w16, h.e16)
        for h in heads:
            row_side = dot(h.xs, h.k16)
            col_side = dot(
                h.xs, jnp.concatenate([low(h.beta * h.k_hat), low(h.q_hat)], axis=0), 0, 0
            )
            d_q = row_side[n:] + h.gain * h.d_qd
            in_term = h.beta * h.gain * h.dr_s
            d_k = h.rk * (h.beta * row_side[:n] - in_term + h.tail * h.d_kt) + col_side
            unit = h.q16.astype(F32) * h.rq
            d_q = h.rq * h.scale * (d_q - unit * jnp.sum(unit * d_q, axis=1, keepdims=True))
            d_k = d_k - h.k_hat * jnp.sum(h.k_hat * d_k, axis=1, keepdims=True)
            dq_ref[:, h.lanes] = low(d_q)
            dk_ref[:, h.lanes] = low(d_k)
            tail_term = h.d_kt * h.k_hat * h.tail
            direct = h.gain * h.d_qd * h.q_hat - in_term * h.k_hat - tail_term
            folded = sum(h.weights[:, i * size : (i + 1) * size] for i in range(n // size))
            row_sum = jnp.sum(folded + direct, axis=1, keepdims=True)
            end = jnp.sum(
                jnp.sum(tail_term, axis=0, keepdims=True)
                + jnp.sum(h.gain_end * (h.s16.astype(F32) * jnp.transpose(h.e16.astype(F32))), axis=0, keepdims=True),
                axis=1, keepdims=True,
            )
            last = lax.broadcasted_iota(jnp.int32, (1, n), 1) == n - 1
            col_acc[h.head : h.head + 1, :] = jnp.where(last, end, 0.0) - jnp.sum(
                h.weights, axis=0, keepdims=True
            )
            row_acc[...] = jnp.where(lane == h.head, row_sum, row_acc[...])
            d_beta = (1.0 - h.beta) * jnp.sum(h.dr * h.written, axis=1, keepdims=True)
            db_acc[...] = jnp.where(lane == h.head, d_beta, db_acc[...])
    d_sums = jnp.transpose(row_acc[...])[0:count] + col_acc[...]
    d_log = dot(d_sums, (rows >= cols).astype(F32), precision=HIGHEST)
    dd_ref[...] = -rate_column(rate_ref) * sigmoid(dp_ref[...]) * d_log
    db_ref[...] = jnp.transpose(db_acc[...])[0:count]


def call(body, name, args, outs, scratch=(), flops=0, anywhere=()):
    def place(i, a):
        space = pltpu.SMEM if a.ndim == 1 else pltpu.HBM if i in anywhere else pltpu.VMEM
        return pl.BlockSpec(memory_space=space)

    results = pl.pallas_call(
        body,
        in_specs=[place(i, a) for i, a in enumerate(args)],
        out_specs=[pl.BlockSpec(memory_space=pltpu.VMEM) for _ in outs],
        out_shape=outs,
        scratch_shapes=list(scratch),
        compiler_params=pltpu.CompilerParams(vmem_limit_bytes=VMEM.get(name, 6) * MIB),
        cost_estimate=pl.CostEstimate(flops=flops, bytes_accessed=1 << 20, transcendentals=0),
    )(*args)
    return list(results)


def shape(*dims, dtype=BF16):
    return jax.ShapeDtypeStruct(dims, dtype)


def total_kernel(maps, total_ref):
    group, _, share = maps.shape[:3]
    for i in range(share):
        g, o, t = maps[group - 1, 1, i], maps[0, 2, i], maps[0, 0, i]
        for j in range(1, group):
            b = group - 1 - j
            g = low(maps[b, 1, i].astype(F32) + dot(g, maps[b, 0, i]))
            o = low(maps[j, 2, i].astype(F32) + dot(maps[j, 0, i], o))
            t = low(dot(maps[j, 0, i], t))
        total_ref[0, i], total_ref[1, i], total_ref[2, i] = t, g, o


def join_kernel(level, last, lead_ref, own, other, out_ref, both):
    lead = lead_ref[0]
    bit = (lead >> level) & 1
    both[bit] = own[...]
    both[1 - bit] = other[...]
    for i in range(own.shape[1]):
        g = low(both[0, 1, i].astype(F32) + dot(both[1, 1, i], both[0, 0, i]))
        o = low(both[1, 2, i].astype(F32) + dot(both[1, 0, i], both[0, 2, i]))
        if last:
            out_ref[i] = jnp.where((lead >> (level + 1)) & 1 == 0, o, g)
        else:
            out_ref[0, i], out_ref[1, i], out_ref[2, i] = low(dot(both[1, 0, i], both[0, 0, i])), g, o


def spread_kernel(levels, lead_ref, pos_ref, maps, *refs):
    ranges, far, out_refs, result = refs[: 2 * levels], refs[2 * levels], refs[2 * levels + 1 : -1], refs[-1]
    lead = lead_ref[0]
    group, _, share = maps.shape[:3]
    later = (lead >> levels) & 1
    zero = jnp.zeros(far.shape[1:], BF16)
    es = [jnp.where(later == 0, far[i], zero) for i in range(share)]
    ss = [jnp.where(later == 0, zero, far[i]) for i in range(share)]
    for level in range(levels - 1, -1, -1):
        other = ranges[2 * level + 1]
        bit = (lead >> level) & 1
        for i in range(share):
            e = low(other[1, i].astype(F32) + dot(es[i], other[0, i]))
            s = low(other[2, i].astype(F32) + dot(other[0, i], ss[i]))
            es[i], ss[i] = jnp.where(bit == 0, e, es[i]), jnp.where(bit == 0, ss[i], s)
    for j in range(group):
        b = group - 1 - j
        for i in range(share):
            result[b, 0, i], result[j, 1, i] = es[i], ss[i]
            if j < group - 1:
                es[i] = low(maps[b, 1, i].astype(F32) + dot(es[i], maps[b, 0, i]))
                ss[i] = low(maps[j, 2, i].astype(F32) + dot(maps[j, 0, i], ss[i]))
    for d, out_ref in enumerate(out_refs):
        out_ref[...] = result[pos_ref[0] ^ d]


def group_size(count, heads):
    size = 1
    while size * size < count and count % (2 * size) == 0 and heads % (2 * size) == 0:
        size *= 2
    return size


def per_device(queries, keys, hidden, value_weight, beta_pre, decay_pre, decay_rate, out_grad):
    heads = decay_rate.shape[0]
    n, width = queries.shape
    dk = width // heads
    dv = value_weight.shape[1] // heads
    model = hidden.shape[1]
    spans = lax.axis_size("sp")
    group = group_size(spans, heads)
    outer = spans // group
    place = lax.axis_index("sp")
    pos = lax.rem(place, group)
    lead = lax.div(place, group)
    lead_arr = jnp.full((1,), lead, jnp.int32)
    pos_arr = jnp.full((1,), pos, jnp.int32)
    share = heads // group
    beta_t, decay_t = beta_pre.T, decay_pre.T
    big = heads * n * n * 256
    teams = [list(range(s, s + group)) for s in range(0, spans, group)]

    def swap(x):
        return lax.all_to_all(x, "sp", 0, 0, axis_index_groups=teams)

    def near(x, d):
        return lax.ppermute(x, "sp", [(s, s ^ d) for s in range(spans)]) if d else x

    def across(x, reach):
        return lax.ppermute(x, "sp", [(s, s ^ (reach * group)) for s in range(spans)])

    rows = model // spans
    col_scratch = [
        pltpu.VMEM((n, 128), F32), pltpu.VMEM((n, 128), F32), pltpu.VMEM((heads, n), F32)
    ]
    maps, inv, dr, y, bdr, by, values, *hidden_t = call(
        functools.partial(local_kernel, PACK, share, outer),
        "local",
        [pos_arr, queries, keys, out_grad, hidden, value_weight, beta_t, decay_t, decay_rate],
        [shape(group, 3, share, dk, dv), shape(heads, n, n)]
        + [shape(n, width)] * 5
        + [shape(outer * rows, n)] * group,
        col_scratch
        + [pltpu.VMEM((n, width), BF16)] * 3
        + [pltpu.VMEM(hidden.shape, BF16), pltpu.VMEM((model, n), BF16), pltpu.VMEM(value_weight.shape, BF16), pltpu.SemaphoreType.DMA((5,))],
        big,
        (1, 2, 3, 4, 5),
    )
    small = group * share * dk * dk * dk * 4
    triple, single = shape(3, share, dk, dv), shape(share, dk, dv)

    maps = swap(maps)
    (total,) = call(total_kernel, "total", [maps], [triple], (), small)
    levels = outer.bit_length() - 2
    ranges = []
    for level in range(levels):
        other = across(total, 1 << level)
        ranges += [total, other]
        last = level == levels - 1
        (total,) = call(
            functools.partial(join_kernel, level, last), "join", [lead_arr, total, other],
            [single if last else triple], [pltpu.VMEM((2,) + triple.shape, BF16)], small,
        )
    far = across(total, 1 << levels)
    moved = []
    for d, part in enumerate(hidden_t):
        moved.append(near(part, d))
    hidden_t = moved
    states = call(
        functools.partial(spread_kernel, levels), "spread", [lead_arr, pos_arr, maps, *ranges, far],
        [shape(2, share, dk, dv)] * group, [pltpu.VMEM((group, 2, share, dk, dv), BF16)], small,
    )
    for d in range(1, group):
        states[d] = near(states[d], d)

    first = max(1, heads * 4 // 8) * dv
    widths = [first, width - first]
    states, d_values, *grad_chunks = call(
        functools.partial(values_kernel, share, group),
        "values",
        [pos_arr, bdr, by, *states],
        [shape(group, 2, share, dk, dv), shape(n, width)] + [shape(n, chunk) for chunk in widths],
        (),
        heads * n * dk * dv * 2,
    )
    pieces = []
    for c, own in enumerate(grad_chunks):
        chunk = widths[c]
        parts = []
        for d in range(group):
            parts.append(near(own, d))
        blocks = call(
            functools.partial(weight_kernel, group, outer),
            "weight",
            [lead_arr, *hidden_t, *parts],
            [shape(rows, chunk, dtype=BF16 if e else F32) for e in range(outer)],
            [pltpu.VMEM((outer * rows, chunk), F32)],
            2 * group * n * outer * rows * chunk,
        )
        for e, block in enumerate(blocks):
            pieces.append(across(block, e) if e else block)
    (d_weight,) = call(
        functools.partial(sum_kernel, outer), "sum", pieces, [shape(rows, width, dtype=F32)], (), rows * width
    )

    core = lax.axis_index("tp")
    cores = lax.axis_size("tp")
    own_rows = n // cores
    shares = call(
        functools.partial(input_kernel, cores), "input",
        [jnp.full((1,), core, jnp.int32), d_values, value_weight],
        [shape(own_rows, model, dtype=BF16 if d else F32) for d in range(cores)],
        [pltpu.VMEM((n, model), F32)], n * width * model * 2,
    )
    shares = [
        lax.ppermute(x, "tp", [(c, (c + d) % cores) for c in range(cores)]) if d else x
        for d, x in enumerate(shares)
    ]
    (d_hidden,) = call(add_kernel, "add", shares, [shape(own_rows, model)], (), own_rows * model)

    d_queries, d_keys, d_beta, d_decay = call(
        functools.partial(grads_kernel, PACK, share),
        "grads",
        [queries, keys, values, out_grad, beta_t, decay_t, decay_rate, inv, dr, y, states],
        [shape(n, width), shape(n, width), shape(heads, n, dtype=F32), shape(heads, n, dtype=F32)],
        col_scratch + [pltpu.VMEM((n, dk), F32), pltpu.VMEM((heads, n), F32), pltpu.VMEM((n, dk), F32)],
        big,
    )
    return (d_queries, d_keys, d_beta.T, d_decay.T, d_hidden, d_weight)


def solution(mesh):
    return jax.shard_map(
        per_device,
        mesh=mesh,
        in_specs=(
            P("sp", "tp"),
            P("sp", "tp"),
            P("sp", None),
            P(None, "tp"),
            P("sp", "tp"),
            P("sp", "tp"),
            P("tp"),
            P("sp", "tp"),
        ),
        out_specs=(
            P("sp", "tp"),
            P("sp", "tp"),
            P("sp", "tp"),
            P("sp", "tp"),
            P(("sp", "tp"), None),
            P("sp", "tp"),
        ),
        check_vma=False,
    )
```
